512 devices in a mesh: grp: 2 (over y), fs: 16 (over z), tp: 16 (over x, core).
Axes of the slice: x: 8, y: 2, z: 16, core: 2. Of those that a mesh axis runs over, the one named last changes fastest.
The devices are a block of a 8x16x16 slice.
Arguments:
- tokens: bfloat16 [8192, 2048], P(('grp', 'fs'), 'tp'), parts along dimension 0, may hold values from -6 to 6
- route_experts: int32 [8192, 2], P(('grp', 'fs')), parts along dimension 0, may hold values from 0 to 15, as said below
- group_weight: float32 [8192], P(('grp', 'fs')), parts along dimension 0, may hold values from 0.2 to 1
- pair_logit: float32 [8192], P(('grp', 'fs')), parts along dimension 0, may hold values from -6 to 6
- norm_gain: float32 [2048], replicated, may hold values from 0.1 to 1.9
- gate_train: float32 [16, 2048, 2048], P(None, 'fs', 'tp'), may hold values from -0.125 to 0.125
- up_train: float32 [16, 2048, 2048], P(None, 'fs', 'tp'), may hold values from -0.125 to 0.125
- down_train: float32 [16, 2048, 2048], P(None, 'fs', 'tp'), may hold values from -0.125 to 0.125
Outputs:
- gate_serve: bfloat16 [32, 2048, 2048], P(('grp', 'fs'), None, 'tp'), parts along dimension 0
- up_serve: bfloat16 [32, 2048, 2048], P(('grp', 'fs'), None, 'tp'), parts along dimension 0
- down_serve: bfloat16 [32, 2048, 2048], P(('grp', 'fs'), None, 'tp'), parts along dimension 0
- moe_out: bfloat16 [8192, 2048], P(('grp', 'fs'), 'tp'), parts along dimension 0
The draws below stay inside these ranges and needn't reach their ends.
There are 2 independent parts, one for each index of `grp`. The reference program is written for one: setup_inputs(seed, part) draws one part's arguments, and reference() takes and returns one part's arrays. A program takes and returns all parts, laid end to end along the dimension named above; an argument that names none is the same for every part. Nothing has to cross between parts.
Inputs may be any that keep to these rules, and one draw needn't show every extreme that they name: `route_experts`: each row names two different experts of the same group of 4 consecutive expert numbers. Among the 256 aligned rows of one index of fs, no expert is named by more than 64 rows, and in every draw some expert is named by exactly 64 rows from every such block.
All inputs are finite; a program needn't handle non-finite values.
Results may differ from the reference program's by a relative error of at most 0.018.
Values may be sent and summed in bfloat16 or wider, within the bound.
A program may use at most 64 MiB of HBM per device.

```python
import math
import jax
import jax.numpy as jnp
from jax import lax

D = 2048
FF = 2048
GROUPS = 4
PER_GROUP = 4
TOK_DEV = 256
EXPERTS = 16
CAP = 64
TOKENS = 4096
N_FS = 16
N_TP = 16


def draw_route_experts(key, part):
    blocks = TOKENS // TOK_DEV
    busiest = jax.random.randint(jax.random.fold_in(key, 7), (), 0, GROUPS)
    block_keys = jax.random.split(jax.random.fold_in(key, 11), blocks)
    group_ids = jnp.arange(GROUPS, dtype=jnp.int32)

    def one_block(block_key):
        cut_key, relabel_key, shuffle_key = jax.random.split(block_key, 3)
        remainder = TOK_DEV - 2 * CAP
        cut_points = jnp.sort(jax.random.randint(cut_key, (2,), 0, remainder + 1))
        others = jnp.stack([cut_points[0], cut_points[1] - cut_points[0], remainder - cut_points[1]])
        other_slot = jnp.minimum((group_ids - busiest - 1) % GROUPS, 2)
        counts = jnp.where(group_ids == busiest, 2 * CAP, others[other_slot])
        group_ends = jnp.cumsum(counts)
        group_starts = group_ends - counts
        positions = jnp.arange(TOK_DEV, dtype=jnp.int32)
        member = jnp.sum((positions[:, None] >= group_ends[None, :]).astype(jnp.int32), axis=1)
        member = jnp.minimum(member, GROUPS - 1)
        within = positions - group_starts[member]
        first_rank = within % PER_GROUP
        second = (first_rank + 1 + within // PER_GROUP % (PER_GROUP - 1)) % PER_GROUP

        def relabel_group(group):
            return jax.random.permutation(jax.random.fold_in(relabel_key, group), PER_GROUP)
        relabel = jax.vmap(relabel_group)(group_ids)
        chosen_pair = jnp.stack([member * PER_GROUP + relabel[member, first_rank], member * PER_GROUP + relabel[member, second]], axis=1)
        shuffle = jax.random.permutation(shuffle_key, TOK_DEV)
        return chosen_pair[shuffle]
    return jax.vmap(one_block)(block_keys).reshape(TOKENS, 2).astype(jnp.int32)


def shard_levels(key, shape, pieces, smallest, high):
    loudness = 1.0
    for position, blocks in pieces:
        draws = jax.random.uniform(jax.random.fold_in(jax.random.fold_in(key, 6), position), (blocks,), jnp.float32, smallest / len(pieces), high / len(pieces))
        loudness = loudness * jnp.repeat(jnp.exp(draws), shape[position] // blocks).reshape((-1,) + (1,) * (len(shape) - 1 - position))
    return loudness


def normal_values(own_key, shape, width, most, shards=(), kind=jnp.bfloat16):
    values = width * jax.random.normal(own_key, shape, jnp.float32)
    if shards:
        values = values * shard_levels(own_key, shape, shards, -0.22, 0.18)
    return jnp.clip(values, -most, most).astype(kind)


def setup_inputs(seed: int = 0, part: int = 0) -> dict:
    streams_of = jax.random.split(jax.random.key(seed), 9)
    own_keys = jax.random.split(jax.random.fold_in(streams_of[8], part), 9)
    return {
        "tokens": normal_values(own_keys[0], (TOKENS, D), 1.0, 6.0, ((0, 16), (1, 16))),
        "route_experts": draw_route_experts(jax.random.fold_in(jax.random.fold_in(streams_of[8], part), 71), part),
        "group_weight": jnp.clip(jnp.exp(math.log(1.0) - 1.609438 * jax.random.uniform(own_keys[2], (TOKENS,), jnp.float32) ** shard_levels(own_keys[2], (TOKENS,), ((0, 16),), -0.2, 0.2)), 0.2, 1.0),
        "pair_logit": normal_values(own_keys[3], (TOKENS,), 1.5, 6.0, ((0, 16),), jnp.float32),
        "norm_gain": jnp.clip(1.0 + 0.18 * jax.random.normal(streams_of[4], (D,), jnp.float32), 0.1, 1.9),
        "gate_train": normal_values(streams_of[5], (EXPERTS, D, FF), D ** -0.5, 0.125, ((1, 16), (2, 16)), jnp.float32),
        "up_train": normal_values(streams_of[6], (EXPERTS, D, FF), D ** -0.5, 0.125, ((1, 16), (2, 16)), jnp.float32),
        "down_train": normal_values(streams_of[7], (EXPERTS, D, FF), FF ** -0.5, 0.125, ((1, 16), (2, 16)), jnp.float32),
    }


def reference(tokens, route_experts, group_weight, pair_logit, norm_gain, gate_train, up_train, down_train):
    gate_serve = (norm_gain[None, :, None] * gate_train).astype(jnp.bfloat16)
    up_serve = (norm_gain[None, :, None] * up_train).astype(jnp.bfloat16)
    down_serve = down_train.astype(jnp.bfloat16)
    as_float = tokens.astype(jnp.float32)
    row_scale = lax.rsqrt(lax.optimization_barrier(jnp.mean(as_float * as_float, axis=1)) + 1e-06)
    first_gate = group_weight * jax.nn.sigmoid(pair_logit)
    second_gate = group_weight * jax.nn.sigmoid(-pair_logit)
    most_rows = N_FS * CAP
    block_width = FF // N_TP

    def add_expert(expert, running):
        first_hit = route_experts[:, 0] == expert
        second_hit = route_experts[:, 1] == expert
        row_weight = jnp.where(first_hit, first_gate, 0.0) + jnp.where(second_hit, second_gate, 0.0)
        sort_key = jnp.where(first_hit | second_hit, 0, 1).astype(jnp.int32)
        row_order = jnp.argsort(sort_key, stable=True)[:most_rows].astype(jnp.int32)
        picked = tokens[row_order]
        picked_scale = row_scale[row_order][:, None]
        gate_pre = picked_scale * jnp.dot(picked, gate_serve[expert], preferred_element_type=jnp.float32)
        up_pre = picked_scale * jnp.dot(picked, up_serve[expert], preferred_element_type=jnp.float32)
        hidden = (jax.nn.silu(gate_pre) * up_pre).astype(jnp.bfloat16)
        down_expert = down_serve[expert]

        def add_block(block, partial_sum):
            column = (block * block_width).astype(jnp.int32)
            hidden_part = lax.dynamic_slice_in_dim(hidden, column, block_width, 1)
            down_part = lax.dynamic_slice_in_dim(down_expert, column, block_width, 1)
            partial_value = jnp.dot(hidden_part, down_part.T, preferred_element_type=jnp.float32).astype(jnp.bfloat16)
            partial_value = lax.optimization_barrier(partial_value)
            return partial_sum + partial_value.astype(jnp.float32)
        summed = lax.fori_loop(0, N_TP, add_block, jnp.zeros((most_rows, D), jnp.float32))
        routed = lax.optimization_barrier(summed.astype(jnp.bfloat16)).astype(jnp.float32)
        return running.at[row_order].add(row_weight[row_order][:, None] * routed)
    total = lax.fori_loop(0, EXPERTS, add_expert, jnp.zeros((TOKENS, D), jnp.float32))
    return (gate_serve, up_serve, down_serve, total.astype(jnp.bfloat16))
```

```python
import functools

import jax
import jax.numpy as jnp
from jax import lax
from jax.experimental import pallas as pl
from jax.experimental.pallas import tpu as pltpu
from jax.sharding import PartitionSpec as P

CAP = 64
MESH = pl.DeviceIdType.MESH
F32 = jnp.float32
BF16 = jnp.bfloat16
CHUNKS = 4


def ring_order(n):
    order = [n // 2]
    for far in range(n // 2 - 1, 0, -1):
        order += [far, n - far]
    return order + [0]


def dot(a, b, dims=(((1,), (0,)), ((), ()))):
    return lax.dot_general(a, b, dims, preferred_element_type=F32)


def body(
    nf,
    nx,
    pair,
    tokens,
    route,
    group_weight,
    pair_logit,
    gain,
    gate_in,
    up_in,
    down_in,
    gate_out,
    up_out,
    down_out,
    moe_out,
    stage_gu,
    stage_d,
    gain_col,
    send_tok,
    send_gu,
    send_d,
    section,
    w_gu,
    dw_own,
    dw_sib,
    h_own,
    h_sib,
    part,
    sums,
    ret,
    back,
    comb,
    sem_in,
    sem_out,
    sem_tok_s,
    sem_tok_r,
    sem_gu_s,
    sem_gu_r,
    sem_d_s,
    sem_d_r,
    sem_y_s,
    sem_y_r,
    sem_x_s,
    sem_x_r,
    sem_c_s,
    sem_c_r,
    sem_h_s,
    sem_h_r,
    sem_w_s,
    sem_w_r,
    sem_q_s,
    sem_q_r,
    sem_b_s,
    sem_b_r,
):
    g, f, t = lax.axis_index("grp"), lax.axis_index("fs"), lax.axis_index("tp")
    x, c = t // 2, t % 2
    half = g % pair
    toks = tokens.shape[0]
    rows_here = gain_col.shape[0]
    rows_half = rows_here // pair
    model = nf * rows_here
    order = ring_order(nf)
    pos = {d: p for p, d in enumerate(order)}
    per = nf // CHUNKS
    chunk_rows = per * CAP
    max_hops = nx // 2

    def hops(ch, way):
        return max_hops - (ch + way) % 2

    def zdev(d):
        return (g, (f + d) % nf, t)

    along = ((g, f, ((x + 1) % nx) * 2 + c), (g, f, ((x + nx - 1) % nx) * 2 + c))
    sib = (g, f, x * 2 + 1 - c)
    twin = (g + 1 - 2 * half, f, t)

    def rows_of(ch):
        return pl.ds(ch * chunk_rows, chunk_rows)

    def remote(src, dst, s, r, dev):
        return pltpu.make_async_remote_copy(
            src_ref=src, dst_ref=dst, send_sem=s, recv_sem=r, device_id=dev, device_id_type=MESH
        )

    def drain(ref, s):
        pltpu.make_async_copy(ref, ref, s).wait()

    mine = pl.ds(half * rows_half, rows_half)
    loads = [
        pltpu.make_async_copy(gate_in.at[:, mine], stage_gu.at[0], sem_in.at[0]),
        pltpu.make_async_copy(up_in.at[:, mine], stage_gu.at[1], sem_in.at[1]),
        pltpu.make_async_copy(down_in.at[:, mine], stage_d, sem_in.at[2]),
    ]
    for cp in loads:
        cp.start()

    barrier = pltpu.get_barrier_semaphore()
    peers = [zdev(d) for d in range(1, nf)] + [along[0], along[1], sib]
    if pair == 2:
        peers.append(twin)
    for dev in peers:
        pl.semaphore_signal(barrier, inc=1, device_id=dev, device_id_type=MESH)

    picked = route[...]
    rel = jnp.where(picked >= f, picked - f, picked - f + nf).astype(F32)
    first = jnp.broadcast_to(rel[:, 0:1], (toks, 128))
    second = jnp.broadcast_to(rel[:, 1:2], (toks, 128))
    first_t = jnp.transpose(first)[0:nf, :]
    second_t = jnp.transpose(second)[0:nf, :]
    offs = lax.broadcasted_iota(jnp.int32, (nf, toks), 0).astype(F32)
    hits_t = (first_t == offs) | (second_t == offs)
    ri = lax.broadcasted_iota(jnp.int32, (toks, toks), 0)
    ci = lax.broadcasted_iota(jnp.int32, (toks, toks), 1)
    upper = jnp.where(ri < ci, 1.0, 0.0).astype(BF16)
    rank_t = dot(jnp.where(hits_t, 1.0, 0.0).astype(BF16), upper)
    slot_t = jnp.where(hits_t, rank_t, -1.0)
    slots = lax.broadcasted_iota(jnp.int32, (CAP, toks), 0).astype(F32)
    for d in range(nf):
        pick = jnp.where(jnp.broadcast_to(slot_t[d : d + 1, :], (CAP, toks)) == slots, 1.0, 0.0)
        got = dot(pick.astype(BF16), tokens[...]).astype(BF16)
        if d == 0:
            section[t, pl.ds(pos[0] * CAP, CAP), :] = got
        else:
            send_tok[pl.ds(pos[d] * CAP, CAP), :] = got

    gain_row = gain[pl.ds(f, 1), :]
    gain_col[...] = jnp.transpose(jnp.broadcast_to(gain_row, (rows_here, rows_here)))
    scale = gain_col[mine, :]
    loads[0].wait()
    loads[1].wait()

    def cast_gu(e, carry):
        send_gu[e, :, 0:128] = (scale * stage_gu[0, e]).astype(BF16)
        send_gu[e, :, 128:256] = (scale * stage_gu[1, e]).astype(BF16)
        return carry

    lax.fori_loop(0, nf, cast_gu, 0)
    pl.semaphore_wait(barrier, len(peers))

    tok_copies = {}
    for d in reversed(order[:-1]):
        there = (nf - d) % nf
        dst = section.at[t, pl.ds(pos[there] * CAP, CAP)]
        ch = pos[there] // per
        tok_copies[d] = remote(
            send_tok.at[pl.ds(pos[d] * CAP, CAP)], dst, sem_tok_s, sem_tok_r.at[ch], zdev(d)
        )
        tok_copies[d].start()

    def w_rows(src):
        return pl.ds(pl.multiple_of(src * rows_here + half * rows_half, rows_half), rows_half)

    def d_at(src):
        return dw_own.at[(src + c) % 2, src // 2, mine]

    for d in order[:-1]:
        remote(
            send_gu.at[(f + d) % nf], w_gu.at[w_rows(f)], sem_gu_s, sem_gu_r.at[(nf - d) % nf], zdev(d)
        ).start()

    w_gu[w_rows(f), :] = send_gu[f]
    if pair == 2:
        remote(send_gu.at[f], w_gu.at[w_rows(f)], sem_y_s.at[0], sem_y_r.at[0], twin).start()

    loads[2].wait()

    def cast_d(e, carry):
        send_d[e] = stage_d[e].astype(BF16)
        return carry

    lax.fori_loop(0, nf, cast_d, 0)
    dw_own[(f + c) % 2, f // 2, mine, :] = send_d[f]

    def pass_gu(d):
        here = w_gu.at[w_rows((f + d) % nf)]
        cp = remote(here, here, sem_y_s.at[0], sem_gu_r.at[d], twin)
        cp.wait_recv()
        if pair == 2:
            remote(here, here, sem_y_s.at[0], sem_y_r.at[0], twin).start()

    def pass_d(d):
        here = d_at((f + d) % nf)
        cp = remote(here, here, sem_y_s.at[1], sem_d_r.at[d], twin)
        cp.wait_recv()
        if pair == 2:
            remote(here, here, sem_y_s.at[1], sem_y_r.at[1], twin).start()

    def gather_send(way, s, ch, blk):
        here = section.at[blk, rows_of(ch)]
        remote(here, here, sem_x_s.at[way], sem_x_r.at[way, s, ch], along[way]).start()

    def gather_share(ch, blk):
        here = section.at[blk, rows_of(ch)]
        remote(here, here, sem_c_s, sem_c_r.at[ch], sib).start()

    waiting = [d for d in order[:-1]]
    first_ch = list(reversed(range(CHUNKS)))
    for k in range(CHUNKS + max_hops):
        for i, ch in enumerate(first_ch):
            s = k - i
            if s == 0:
                count = per - (1 if pos[0] // per == ch else 0)
                drain(send_tok.at[pl.ds(0, count * CAP)], sem_tok_r.at[ch])
                for way in range(2):
                    gather_send(way, 0, ch, t)
                gather_share(ch, t)
            elif 1 <= s <= max_hops:
                for way in range(2):
                    if s > hops(ch, way):
                        continue
                    from_x = (x + (nx - s if way == 0 else s)) % nx
                    blk = from_x * 2 + c
                    here = section.at[blk, rows_of(ch)]
                    remote(
                        here, here, sem_x_s.at[way], sem_x_r.at[way, s - 1, ch], along[way]
                    ).wait_recv()
                    if s < hops(ch, way):
                        gather_send(way, s, ch, blk)
                    gather_share(ch, blk)
                if waiting:
                    pass_gu(waiting.pop(0))

    for d in order[:-1]:
        remote(
            send_d.at[(f + d) % nf], d_at(f), sem_d_s, sem_d_r.at[(nf - d) % nf], zdev(d)
        ).start()
    if pair == 2:
        remote(send_d.at[f], d_at(f), sem_y_s.at[1], sem_y_r.at[1], twin).start()
    while waiting:
        pass_gu(waiting.pop(0))

    lane = lax.broadcasted_iota(jnp.int32, (toks, 128), 1)
    lower = jnp.where(ci < ri, 1.0, 0.0).astype(BF16)
    weight = jnp.transpose(jnp.broadcast_to(group_weight[...], (128, toks)))
    logit = jnp.transpose(jnp.broadcast_to(pair_logit[...], (128, toks)))
    gate_a = weight * jax.nn.sigmoid(logit)
    gate_b = weight * jax.nn.sigmoid(-logit)
    lane_off = jnp.where(lane < CAP, 0, 1).astype(F32)
    lane_slot = jnp.where(lane < CAP, lane, lane - CAP).astype(F32)
    for k in range(nf // 2):
        off = lane_off + 2.0 * k
        is_a, is_b = first == off, second == off
        rank = dot(lower, jnp.where(is_a | is_b, 1.0, 0.0).astype(BF16))
        val = jnp.where(is_a, gate_a, 0.0) + jnp.where(is_b, gate_b, 0.0)
        val = jnp.where(rank == lane_slot, val, 0.0)
        high = val.astype(BF16)
        comb[0, :, pl.ds(k * 128, 128)] = high
        comb[1, :, pl.ds(k * 128, 128)] = (val - high.astype(F32)).astype(BF16)

    if pair == 2:
        drain(w_gu.at[pl.ds(0, nf * rows_half)], sem_y_r.at[0])
    outs = [
        pltpu.make_async_copy(w_gu.at[:, pl.ds(0, 128)], gate_out, sem_out.at[0]),
        pltpu.make_async_copy(w_gu.at[:, pl.ds(128, 128)], up_out, sem_out.at[1]),
        pltpu.make_async_copy(dw_own.at[0], down_out.at[:, c], sem_out.at[2]),
        pltpu.make_async_copy(dw_own.at[1], down_out.at[:, 1 - c], sem_out.at[3]),
    ]
    outs[0].start()
    outs[1].start()

    for ch in range(CHUNKS):
        drain(section.at[pl.ds(0, nx), pl.ds(0, chunk_rows)], sem_c_r.at[ch])
        blocks = [section[j, rows_of(ch), :] for j in range(2 * nx)]
        squares = jnp.zeros((chunk_rows, 128), F32)
        for b in blocks:
            wide = b.astype(F32)
            squares = squares + wide * wide
        row_scale = lax.rsqrt(jnp.sum(squares, axis=1, keepdims=True) / model + 1e-6)
        pre = dot(jnp.concatenate(blocks, axis=1), w_gu[...])
        gate = row_scale * pre[:, 0:128]
        up = row_scale * pre[:, 128:256]
        h_own[rows_of(ch), :] = (gate / (1.0 + jnp.exp(-gate)) * up).astype(BF16)
        remote(
            h_own.at[rows_of(ch)], h_sib.at[rows_of(ch)], sem_h_s, sem_h_r.at[ch], sib
        ).start()

    for d in order[:-1]:
        pass_d(d)
    if pair == 2:
        drain(dw_own.at[0, :, pl.ds(0, nf * rows_half // nx)], sem_y_r.at[1])
    share = remote(dw_own.at[1], dw_sib, sem_w_s, sem_w_r, sib)
    share.start()
    outs[2].start()
    outs[3].start()
    share.wait_recv()

    def sum_send(way, s, ch, src):
        remote(
            src, sums.at[way, s, rows_of(ch)], sem_q_s.at[way], sem_q_r.at[way, s, ch], along[way]
        ).start()

    def target(way, ch, s):
        left = hops(ch, way) - s
        return (x + (left if way == 0 else nx - left)) % nx

    feats = nx * 128
    for ch in range(CHUNKS):
        remote(
            h_own.at[rows_of(ch)], h_sib.at[rows_of(ch)], sem_h_s, sem_h_r.at[ch], sib
        ).wait_recv()
        both = jnp.concatenate([h_own[rows_of(ch), :], h_sib[rows_of(ch), :]], axis=1)
        down = jnp.concatenate(
            [dw_own[0].reshape(feats, 128), dw_sib[...].reshape(feats, 128)], axis=1
        )
        res = dot(both, down, (((1,), (1,)), ((), ()))).astype(BF16)
        for i in range(nx):
            part[i, rows_of(ch), :] = res[:, i * 128 : (i + 1) * 128]
        for way in range(2):
            sum_send(way, 0, ch, part.at[target(way, ch, 0), rows_of(ch)])

    for s in range(1, max_hops + 1):
        for ch in range(CHUNKS):
            for way in range(2):
                last = hops(ch, way)
                if s > last:
                    continue
                here = sums.at[way, s - 1, rows_of(ch)]
                remote(here, here, sem_q_s.at[way], sem_q_r.at[way, s - 1, ch], along[way]).wait_recv()
                if s < last:
                    sums[way, s - 1, rows_of(ch), :] = (
                        sums[way, s - 1, rows_of(ch), :].astype(F32)
                        + part[target(way, ch, s), rows_of(ch), :].astype(F32)
                    ).astype(BF16)
                    sum_send(way, s, ch, here)
            if s == max_hops:
                total = part[x, rows_of(ch), :].astype(F32)
                for way in range(2):
                    total = total + sums[way, hops(ch, way) - 1, rows_of(ch), :].astype(F32)
                ret[rows_of(ch), :] = total.astype(BF16)
                for d in order[ch * per : (ch + 1) * per]:
                    src = ret.at[pl.ds(pos[d] * CAP, CAP)]
                    if d == 0:
                        back[pl.ds(0, CAP), :] = ret[pl.ds(pos[0] * CAP, CAP), :]
                    else:
                        remote(
                            src,
                            back.at[pl.ds(((nf - d) % nf) * CAP, CAP)],
                            sem_b_s,
                            sem_b_r,
                            zdev(d),
                        ).start()

    drain(back.at[pl.ds(0, (nf - 1) * CAP)], sem_b_r)
    rows_back = back[...]
    moe_out[...] = (dot(comb[0], rows_back) + dot(comb[1], rows_back)).astype(BF16)

    for cp in outs:
        cp.wait()
    drain(send_tok.at[pl.ds(0, (nf - 1) * CAP)], sem_tok_s)
    drain(send_gu.at[pl.ds(0, nf - 1)], sem_gu_s)
    drain(send_d.at[pl.ds(0, nf - 1)], sem_d_s)
    if pair == 2:
        drain(send_gu, sem_y_s.at[0])
        drain(send_d, sem_y_s.at[1])
    for way in range(2):
        moved = sum(hops(ch, way) for ch in range(CHUNKS))
        drain(section.at[pl.ds(0, moved), pl.ds(0, chunk_rows)], sem_x_s.at[way])
        drain(section.at[pl.ds(0, moved), pl.ds(0, chunk_rows)], sem_q_s.at[way])
    drain(section.at[pl.ds(0, nx)], sem_c_s)
    drain(h_own, sem_h_s)
    share.wait_send()
    drain(ret.at[pl.ds(0, (nf - 1) * CAP)], sem_b_s)


def shards(
    nf, nt, pair, tokens, route, group_weight, pair_logit, norm_gain, gate_train, up_train, down_train
):
    nx = nt // 2
    toks, width = tokens.shape
    rows_here, units = gate_train.shape[1], gate_train.shape[2]
    rows_half = rows_here // pair
    model = norm_gain.shape[0]
    slots = nf * CAP
    max_hops = nx // 2
    vmem = pl.BlockSpec(memory_space=pltpu.VMEM)
    hbm = pl.BlockSpec(memory_space=pl.ANY)
    dma = pltpu.SemaphoreType.DMA
    gate_serve, up_serve, down_serve, moe = pl.pallas_call(
        functools.partial(body, nf, nx, pair),
        out_shape=(
            jax.ShapeDtypeStruct((model, units), BF16),
            jax.ShapeDtypeStruct((model, units), BF16),
            jax.ShapeDtypeStruct((nx, 2, rows_here, units), BF16),
            jax.ShapeDtypeStruct((toks, width), BF16),
        ),
        in_specs=[vmem] * 5 + [hbm] * 3,
        out_specs=(hbm, hbm, hbm, vmem),
        scratch_shapes=[
            pltpu.VMEM((2, nf, rows_half, units), F32),
            pltpu.VMEM((nf, rows_half, units), F32),
            pltpu.VMEM((rows_here, 128), F32),
            pltpu.VMEM((slots, width), BF16),
            pltpu.VMEM((nf, rows_half, 2 * units), BF16),
            pltpu.VMEM((nf, rows_half, units), BF16),
            pltpu.VMEM((nt, slots, width), BF16),
            pltpu.VMEM((model, 2 * units), BF16),
            pltpu.VMEM((2, nx, rows_here, units), BF16),
            pltpu.VMEM((nx, rows_here, units), BF16),
            pltpu.VMEM((slots, units), BF16),
            pltpu.VMEM((slots, units), BF16),
            pltpu.VMEM((nx, slots, width), BF16),
            pltpu.VMEM((2, max_hops, slots, width), BF16),
            pltpu.VMEM((slots, width), BF16),
            pltpu.VMEM((slots, width), BF16),
            pltpu.VMEM((2, toks, slots), BF16),
            dma((3,)),
            dma((4,)),
            dma,
            dma((CHUNKS,)),
            dma,
            dma((nf,)),
            dma,
            dma((nf,)),
            dma((2,)),
            dma((2,)),
            dma((2,)),
            dma((2, max_hops, CHUNKS)),
            dma,
            dma((CHUNKS,)),
            dma,
            dma((CHUNKS,)),
            dma,
            dma,
            dma((2,)),
            dma((2, max_hops, CHUNKS)),
            dma,
            dma,
        ],
        compiler_params=pltpu.CompilerParams(
            collective_id=0, has_side_effects=True, vmem_limit_bytes=60 * 1024 * 1024
        ),
        name="handover",
    )(
        tokens,
        route,
        group_weight.reshape(1, toks),
        pair_logit.reshape(1, toks),
        norm_gain.reshape(nf, rows_here),
        gate_train,
        up_train,
        down_train,
    )
    return (
        gate_serve.reshape(1, model, units),
        up_serve.reshape(1, model, units),
        down_serve.reshape(1, model, units),
        moe,
    )


def solution(mesh):
    nf, nt = mesh.shape["fs"], mesh.shape["tp"]
    pair = 2 if mesh.shape["grp"] % 2 == 0 else 1
    return jax.shard_map(
        functools.partial(shards, nf, nt, pair),
        mesh=mesh,
        in_specs=(
            P(("grp", "fs"), "tp"),
            P(("grp", "fs"), None),
            P(("grp", "fs")),
            P(("grp", "fs")),
            P(),
            P(None, "fs", "tp"),
            P(None, "fs", "tp"),
            P(None, "fs", "tp"),
        ),
        out_specs=(
            P(("grp", "fs"), None, "tp"),
            P(("grp", "fs"), None, "tp"),
            P(("grp", "fs"), None, "tp"),
            P(("grp", "fs"), "tp"),
        ),
        check_vma=False,
    )
```

```python
import functools

import jax
import jax.numpy as jnp
from jax import lax
from jax.experimental import pallas as pl
from jax.experimental.pallas import tpu as pltpu
from jax.sharding import PartitionSpec as P

CAP = 64
MESH = pl.DeviceIdType.MESH
F32 = jnp.float32
BF16 = jnp.bfloat16
CHUNKS = 4
PASS_FROM = 5
EARLY = 4
SUMS = 8
WAIT = (0, 0, 0, 0, 2, 2, 2, 2)


def ring_order(n):
    order = [n // 2]
    for far in range(n // 2 - 1, 0, -1):
        order += [far, n - far]
    return order + [0]


def dot(a, b, dims=(((1,), (0,)), ((), ()))):
    return lax.dot_general(a, b, dims, preferred_element_type=F32)


def body(
    nf,
    nx,
    pair,
    tokens_in,
    route_in,
    group_weight_in,
    pair_logit_in,
    gain_in,
    gate_in,
    up_in,
    down_in,
    gate_out,
    up_out,
    down_out,
    moe_out,
    tokens,
    route,
    group_weight,
    pair_logit,
    gain,
    stage_gu,
    stage_d,
    gain_col,
    send_tok,
    send_gu,
    send_d,
    section,
    w_gu,
    dw_own,
    dw_sib,
    h_own,
    h_sib,
    part,
    sums,
    ret,
    back,
    comb,
    ready,
    near,
    sem_in,
    sem_out,
    sem_tok_s,
    sem_tok_r,
    sem_gu_s,
    sem_gu_r,
    sem_d_s,
    sem_d_r,
    sem_y_s,
    sem_y_r,
    sem_x_s,
    sem_x_r,
    sem_c_s,
    sem_c_r,
    sem_h_s,
    sem_h_r,
    sem_w_s,
    sem_w_r,
    sem_q_s,
    sem_q_r,
    sem_b_s,
    sem_b_r,
):
    g, f, t = lax.axis_index("grp"), lax.axis_index("fs"), lax.axis_index("tp")
    x, c = t // 2, t % 2
    half = g % pair
    toks = tokens.shape[0]
    rows_here = gain_col.shape[0]
    rows_half = rows_here // pair
    model = nf * rows_here
    order = ring_order(nf)
    pos = {d: p for p, d in enumerate(order)}
    per = nf // CHUNKS
    chunk_rows = per * CAP
    max_hops = nx // 2

    def hops(ch, way):
        return max_hops - (ch + way) % 2

    def zdev(d):
        return (g, (f + d) % nf, t)

    along = ((g, f, ((x + 1) % nx) * 2 + c), (g, f, ((x + nx - 1) % nx) * 2 + c))
    sib = (g, f, x * 2 + 1 - c)
    twin = (g + 1 - 2 * half, f, t)

    def rows_of(ch):
        return pl.ds(ch * chunk_rows, chunk_rows)

    def remote(src, dst, s, r, dev):
        return pltpu.make_async_remote_copy(
            src_ref=src, dst_ref=dst, send_sem=s, recv_sem=r, device_id=dev, device_id_type=MESH
        )

    def drain(ref, s):
        pltpu.make_async_copy(ref, ref, s).wait()

    mine = pl.ds(half * rows_half, rows_half)
    small = [
        pltpu.make_async_copy(src, dst, sem_in.at[3 + i])
        for i, (src, dst) in enumerate(
            (
                (tokens_in, tokens),
                (route_in, route),
                (gain_in, gain),
                (group_weight_in, group_weight),
                (pair_logit_in, pair_logit),
            )
        )
    ]
    for cp in small:
        cp.start()
    loads = [
        pltpu.make_async_copy(gate_in.at[:, mine], stage_gu.at[0], sem_in.at[0]),
        pltpu.make_async_copy(up_in.at[:, mine], stage_gu.at[1], sem_in.at[1]),
        pltpu.make_async_copy(down_in.at[:, mine], stage_d, sem_in.at[2]),
    ]
    for cp in loads:
        cp.start()

    groups = lax.axis_size("grp")
    nt = 2 * nx
    late_first = ((groups - g) // groups) * ((nt - t) // nt)
    rank = (f + nf - late_first) % nf
    later_right = (x + 1) // nx
    earlier_left = (nx - x) // nx
    barrier = pltpu.get_barrier_semaphore()

    def greet(dev):
        pl.semaphore_signal(barrier, inc=1, device_id=dev, device_id_type=MESH)

    def tell(sem, dev):
        pl.semaphore_signal(sem, inc=1, device_id=dev, device_id_type=MESH)

    def if_later(d):
        return pl.when(rank + d < nf)

    def if_earlier(d):
        return pl.when(rank + d >= nf)

    for d in range(1, nf):
        if_later(d)(lambda d=d: greet(zdev(d)))
    pl.when(later_right == 1)(lambda: greet(along[0]))
    pl.when(earlier_left == 0)(lambda: greet(along[1]))
    pl.when(c == 1)(lambda: greet(sib))
    before = rank + (1 - later_right) + earlier_left + (1 - c)
    if pair == 2:
        pl.when(half == 1)(lambda: greet(twin))
        before = before + (1 - half)

    @pl.when(before > 0)
    def _():
        pl.semaphore_wait(barrier, before)

    for d in range(1, nf):
        if_earlier(d)(lambda d=d: tell(ready.at[nf - d], zdev(d)))
    pl.when(later_right == 0)(lambda: tell(near.at[1], along[0]))
    pl.when(earlier_left == 1)(lambda: tell(near.at[0], along[1]))
    pl.when(c == 0)(lambda: tell(near.at[2], sib))
    if pair == 2:
        pl.when(half == 0)(lambda: tell(near.at[3], twin))

    for cp in small:
        cp.wait()
    picked = route[...]
    rel = jnp.where(picked >= f, picked - f, picked - f + nf).astype(F32)
    first_t = jnp.broadcast_to(rel[0:1, :], (nf, toks))
    second_t = jnp.broadcast_to(rel[1:2, :], (nf, toks))
    offs = lax.broadcasted_iota(jnp.int32, (nf, toks), 0).astype(F32)
    hits_t = (first_t == offs) | (second_t == offs)
    ri = lax.broadcasted_iota(jnp.int32, (toks, toks), 0)
    ci = lax.broadcasted_iota(jnp.int32, (toks, toks), 1)
    upper = jnp.where(ri < ci, 1.0, 0.0).astype(BF16)
    rank_t = dot(jnp.where(hits_t, 1.0, 0.0).astype(BF16), upper)
    slot_t = jnp.where(hits_t, rank_t, -1.0)
    slots = lax.broadcasted_iota(jnp.int32, (CAP, toks), 0).astype(F32)
    for d in range(nf):
        pick = jnp.where(jnp.broadcast_to(slot_t[d : d + 1, :], (CAP, toks)) == slots, 1.0, 0.0)
        got = dot(pick.astype(BF16), tokens[...]).astype(BF16)
        if d == 0:
            section[t, pl.ds(pos[0] * CAP, CAP), :] = got
        else:
            send_tok[pl.ds(pos[d] * CAP, CAP), :] = got

    def w_rows(src):
        return pl.ds(pl.multiple_of(src * rows_here + half * rows_half, rows_half), rows_half)

    def d_at(src):
        return dw_own.at[(src + c) % 2, src // 2, mine]

    def send_rows(d):
        there = pos[(nf - d) % nf]
        remote(
            send_tok.at[pl.ds(pos[d] * CAP, CAP)],
            section.at[t, pl.ds(there * CAP, CAP)],
            sem_tok_s,
            sem_tok_r.at[there // per],
            zdev(d),
        ).start()

    def send_gate_up(d):
        remote(
            send_gu.at[(f + d) % nf], w_gu.at[w_rows(f)], sem_gu_s, sem_gu_r.at[f], zdev(d)
        ).start()

    def send_down(d):
        remote(
            send_d.at[(f + d) % nf], d_at(f), sem_d_s, sem_d_r.at[f], zdev(d)
        ).start()

    for d in order[:-1]:
        if_earlier(d)(lambda d=d: send_rows(d))

    gain_row = gain[pl.ds(f, 1), :]
    gain_col[...] = jnp.transpose(jnp.broadcast_to(gain_row, (rows_here, rows_here)))
    scale = gain_col[mine, :]
    loads[0].wait()
    loads[1].wait()

    def cast_gu(e, carry):
        send_gu[e, :, 0:128] = (scale * stage_gu[0, e]).astype(BF16)
        send_gu[e, :, 128:256] = (scale * stage_gu[1, e]).astype(BF16)
        return carry

    lax.fori_loop(0, nf, cast_gu, 0)
    w_gu[w_rows(f), :] = send_gu[f]
    loads[2].wait()

    def cast_d(e, carry):
        send_d[e] = stage_d[e].astype(BF16)
        return carry

    lax.fori_loop(0, nf, cast_d, 0)
    dw_own[(f + c) % 2, f // 2, mine, :] = send_d[f]

    first_in = nf // 2 + EARLY

    def send_weights(d):
        send_gate_up(d)
        send_down(d)

    def if_early(d):
        return pl.when((rank < first_in) & ((rank + d < first_in) | (rank + d >= nf)))

    def late(d):
        return (rank >= first_in) | ((rank + d < nf) & (rank + d >= first_in))

    def if_late(d):
        return pl.when(late(d))

    for d in order[:-1]:
        pl.when((rank + d >= nf) & (rank < first_in))(lambda d=d: send_weights(d))
    for d in range(1, nf):

        @if_later(d)
        def _(d=d):
            pl.semaphore_wait(ready.at[d], 1)
            send_rows(d)

        pl.when(rank + d < first_in)(lambda d=d: send_weights(d))

    def burst(guard):
        for step in (send_gate_up, send_down):
            for d in order[:-1]:
                pl.when(guard(d))(lambda d=d, step=step: step(d))

    burst(lambda d: rank == nf - 1)

    @pl.when(later_right == 1)
    def _():
        pl.semaphore_wait(near.at[0], 1)

    @pl.when(earlier_left == 0)
    def _():
        pl.semaphore_wait(near.at[1], 1)

    @pl.when(c == 1)
    def _():
        pl.semaphore_wait(near.at[2], 1)

    if pair == 2:

        @pl.when(half == 1)
        def _():
            pl.semaphore_wait(near.at[3], 1)

        remote(send_gu.at[f], w_gu.at[w_rows(f)], sem_y_s.at[0], sem_y_r.at[0], twin).start()
        remote(send_d.at[f], d_at(f), sem_y_s.at[1], sem_y_r.at[1], twin).start()

    def pass_gu(d):
        src = (f + d) % nf
        here = w_gu.at[w_rows(src)]
        remote(here, here, sem_y_s.at[0], sem_gu_r.at[src], twin).wait_recv()
        if pair == 2:
            remote(here, here, sem_y_s.at[0], sem_y_r.at[0], twin).start()

    def pass_d(d):
        src = (f + d) % nf
        here = d_at(src)
        remote(here, here, sem_y_s.at[1], sem_d_r.at[src], twin).wait_recv()
        if pair == 2:
            remote(here, here, sem_y_s.at[1], sem_y_r.at[1], twin).start()

    def gather_send(way, s, ch, blk):
        here = section.at[blk, rows_of(ch)]
        remote(here, here, sem_x_s.at[way], sem_x_r.at[way, s, ch], along[way]).start()

    def gather_share(ch, blk):
        here = section.at[blk, rows_of(ch)]
        remote(here, here, sem_c_s, sem_c_r.at[ch], sib).start()

    def gather_own(ch):
        count = per - (1 if pos[0] // per == ch else 0)
        drain(send_tok.at[pl.ds(0, count * CAP)], sem_tok_r.at[ch])
        for way in range(2):
            gather_send(way, 0, ch, t)
        gather_share(ch, t)

    def gather_step(s, ch):
        for way in range(2):
            if s > hops(ch, way):
                continue
            from_x = (x + (nx - s if way == 0 else s)) % nx
            blk = from_x * 2 + c
            here = section.at[blk, rows_of(ch)]
            remote(
                here, here, sem_x_s.at[way], sem_x_r.at[way, s - 1, ch], along[way]
            ).wait_recv()
            if s < hops(ch, way):
                gather_send(way, s, ch, blk)
            gather_share(ch, blk)

    def hidden(ch):
        drain(section.at[pl.ds(0, nx), pl.ds(0, chunk_rows)], sem_c_r.at[ch])
        blocks = [section[j, rows_of(ch), :] for j in range(2 * nx)]
        squares = jnp.zeros((chunk_rows, 128), F32)
        for b in blocks:
            wide = b.astype(F32)
            squares = squares + wide * wide
        row_scale = lax.rsqrt(jnp.sum(squares, axis=1, keepdims=True) / model + 1e-6)
        pre = dot(jnp.concatenate(blocks, axis=1), w_gu[...])
        gate = row_scale * pre[:, 0:128]
        up = row_scale * pre[:, 128:256]
        h_own[rows_of(ch), :] = (gate / (1.0 + jnp.exp(-gate)) * up).astype(BF16)
        remote(
            h_own.at[rows_of(ch)], h_sib.at[rows_of(ch)], sem_h_s, sem_h_r.at[ch], sib
        ).start()

    sum_rows = nf * CAP // SUMS
    per_sum = nf // SUMS

    def srows(u):
        return pl.ds(u * sum_rows, sum_rows)

    def sum_send(way, s, u, src):
        remote(
            src, sums.at[way, s, srows(u)], sem_q_s.at[way], sem_q_r.at[way, s, u], along[way]
        ).start()

    def target(way, u, s):
        left = hops(u, way) - s
        return (x + (left if way == 0 else nx - left)) % nx

    feats = nx * 128

    def partials(ch):
        remote(
            h_own.at[rows_of(ch)], h_sib.at[rows_of(ch)], sem_h_s, sem_h_r.at[ch], sib
        ).wait_recv()
        both = jnp.concatenate([h_own[rows_of(ch), :], h_sib[rows_of(ch), :]], axis=1)
        down = jnp.concatenate(
            [dw_own[0].reshape(feats, 128), dw_sib[...].reshape(feats, 128)], axis=1
        )
        res = dot(both, down, (((1,), (1,)), ((), ()))).astype(BF16)
        for i in range(nx):
            part[i, rows_of(ch), :] = res[:, i * 128 : (i + 1) * 128]

    def sum_step(s, u):
        for way in range(2):
            last = hops(u, way)
            if s > last:
                continue
            if s == 0:
                sum_send(way, 0, u, part.at[target(way, u, 0), srows(u)])
                continue
            here = sums.at[way, s - 1, srows(u)]
            remote(here, here, sem_q_s.at[way], sem_q_r.at[way, s - 1, u], along[way]).wait_recv()
            if s < last:
                sums[way, s - 1, srows(u), :] = (
                    sums[way, s - 1, srows(u), :].astype(F32)
                    + part[target(way, u, s), srows(u), :].astype(F32)
                ).astype(BF16)
                sum_send(way, s, u, here)
        if s < max_hops:
            return
        total = part[x, srows(u), :].astype(F32)
        for way in range(2):
            total = total + sums[way, hops(u, way) - 1, srows(u), :].astype(F32)
        ret[srows(u), :] = total.astype(BF16)
        for d in order[u * per_sum : (u + 1) * per_sum]:
            if d == 0:
                back[pl.ds(0, CAP), :] = ret[pl.ds(pos[0] * CAP, CAP), :]
            else:
                remote(
                    ret.at[pl.ds(pos[d] * CAP, CAP)],
                    back.at[pl.ds(((nf - d) % nf) * CAP, CAP)],
                    sem_b_s,
                    sem_b_r,
                    zdev(d),
                ).start()

    for ch in reversed(range(CHUNKS)):
        gather_own(ch)

    burst(lambda d: (rank < nf - 1) & late(d))
    for step in (pass_gu, pass_d):
        for d in order[:-1]:
            if_early(d)(lambda d=d, step=step: step(d))
    waiting = [(step, d) for step in (pass_gu, pass_d) for d in order[:-1]]
    event = 0
    for s in range(1, max_hops + 1):
        for ch in reversed(range(CHUNKS)):
            gather_step(s, ch)
            event += 1
            if event > PASS_FROM:
                for step, d in (waiting.pop(0), waiting.pop(0)):
                    if_late(d)(functools.partial(step, d))
    outs = [
        pltpu.make_async_copy(w_gu.at[:, pl.ds(0, 128)], gate_out, sem_out.at[0]),
        pltpu.make_async_copy(w_gu.at[:, pl.ds(128, 128)], up_out, sem_out.at[1]),
        pltpu.make_async_copy(dw_own.at[0], down_out.at[:, c], sem_out.at[2]),
        pltpu.make_async_copy(dw_own.at[1], down_out.at[:, 1 - c], sem_out.at[3]),
    ]
    while waiting and waiting[0][0] is pass_gu:
        step, d = waiting.pop(0)
        if_late(d)(lambda: step(d))
    if pair == 2:
        drain(w_gu.at[pl.ds(0, nf * rows_half)], sem_y_r.at[0])
    outs[0].start()
    outs[1].start()
    for ch in range(CHUNKS):
        hidden(ch)
    for step, d in waiting:
        if_late(d)(lambda: step(d))
    if pair == 2:
        drain(dw_own.at[0, :, pl.ds(0, nf * rows_half // nx)], sem_y_r.at[1])
    share = remote(dw_own.at[1], dw_sib, sem_w_s, sem_w_r, sib)
    share.start()
    outs[2].start()
    outs[3].start()
    share.wait_recv()
    for ch in range(CHUNKS):
        partials(ch)
        for u in range(ch * SUMS // CHUNKS, (ch + 1) * SUMS // CHUNKS):
            if WAIT[u] == 0:
                sum_step(0, u)

    lane = lax.broadcasted_iota(jnp.int32, (toks, 128), 1)
    lower = jnp.where(ci < ri, 1.0, 0.0).astype(BF16)
    first = jnp.transpose(jnp.broadcast_to(rel[0:1, :], (128, toks)))
    second = jnp.transpose(jnp.broadcast_to(rel[1:2, :], (128, toks)))
    weight = jnp.transpose(jnp.broadcast_to(group_weight[...], (128, toks)))
    logit = jnp.transpose(jnp.broadcast_to(pair_logit[...], (128, toks)))
    gate_a = weight * jax.nn.sigmoid(logit)
    gate_b = weight * jax.nn.sigmoid(-logit)
    lane_off = jnp.where(lane < CAP, 0, 1).astype(F32)
    lane_slot = jnp.where(lane < CAP, lane, lane - CAP).astype(F32)
    for k in range(nf // 2):
        off = lane_off + 2.0 * k
        is_a, is_b = first == off, second == off
        seen = dot(lower, jnp.where(is_a | is_b, 1.0, 0.0).astype(BF16))
        val = jnp.where(is_a, gate_a, 0.0) + jnp.where(is_b, gate_b, 0.0)
        val = jnp.where(seen == lane_slot, val, 0.0)
        high = val.astype(BF16)
        comb[0, :, pl.ds(k * 128, 128)] = high
        comb[1, :, pl.ds(k * 128, 128)] = (val - high.astype(F32)).astype(BF16)

    for k in range(1, max_hops + 1 + max(WAIT)):
        for u in range(SUMS):
            s = k - WAIT[u]
            if 0 <= s <= max_hops:
                sum_step(s, u)

    drain(back.at[pl.ds(0, (nf - 1) * CAP)], sem_b_r)
    rows_back = back[...]
    moe_out[...] = (dot(comb[0], rows_back) + dot(comb[1], rows_back)).astype(BF16)

    for cp in outs:
        cp.wait()
    drain(send_tok.at[pl.ds(0, (nf - 1) * CAP)], sem_tok_s)
    drain(send_gu.at[pl.ds(0, nf - 1)], sem_gu_s)
    drain(send_d.at[pl.ds(0, nf - 1)], sem_d_s)
    if pair == 2:
        drain(send_gu, sem_y_s.at[0])
        drain(send_d, sem_y_s.at[1])
    for way in range(2):
        moved = sum(hops(ch, way) for ch in range(CHUNKS))
        drain(section.at[pl.ds(0, moved), pl.ds(0, chunk_rows)], sem_x_s.at[way])
        moved = sum(hops(u, way) for u in range(SUMS))
        drain(section.at[pl.ds(0, nx // 2), pl.ds(0, moved * sum_rows // (nx // 2))], sem_q_s.at[way])
    drain(section.at[pl.ds(0, nx)], sem_c_s)
    drain(h_own, sem_h_s)
    share.wait_send()
    drain(ret.at[pl.ds(0, (nf - 1) * CAP)], sem_b_s)


def shards(
    nf, nt, pair, tokens, route, group_weight, pair_logit, norm_gain, gate_train, up_train, down_train
):
    nx = nt // 2
    toks, width = tokens.shape
    rows_here, units = gate_train.shape[1], gate_train.shape[2]
    rows_half = rows_here // pair
    model = norm_gain.shape[0]
    slots = nf * CAP
    max_hops = nx // 2
    vmem = pl.BlockSpec(memory_space=pltpu.VMEM)
    hbm = pl.BlockSpec(memory_space=pl.ANY)
    dma = pltpu.SemaphoreType.DMA
    gate_serve, up_serve, down_serve, moe = pl.pallas_call(
        functools.partial(body, nf, nx, pair),
        out_shape=(
            jax.ShapeDtypeStruct((model, units), BF16),
            jax.ShapeDtypeStruct((model, units), BF16),
            jax.ShapeDtypeStruct((nx, 2, rows_here, units), BF16),
            jax.ShapeDtypeStruct((toks, width), BF16),
        ),
        in_specs=[hbm] * 8,
        out_specs=(hbm, hbm, hbm, vmem),
        scratch_shapes=[
            pltpu.VMEM((toks, width), BF16),
            pltpu.VMEM((2, toks), jnp.int32),
            pltpu.VMEM((1, toks), F32),
            pltpu.VMEM((1, toks), F32),
            pltpu.VMEM((nf, rows_here), F32),
            pltpu.VMEM((2, nf, rows_half, units), F32),
            pltpu.VMEM((nf, rows_half, units), F32),
            pltpu.VMEM((rows_here, 128), F32),
            pltpu.VMEM((slots, width), BF16),
            pltpu.VMEM((nf, rows_half, 2 * units), BF16),
            pltpu.VMEM((nf, rows_half, units), BF16),
            pltpu.VMEM((nt, slots, width), BF16),
            pltpu.VMEM((model, 2 * units), BF16),
            pltpu.VMEM((2, nx, rows_here, units), BF16),
            pltpu.VMEM((nx, rows_here, units), BF16),
            pltpu.VMEM((slots, units), BF16),
            pltpu.VMEM((slots, units), BF16),
            pltpu.VMEM((nx, slots, width), BF16),
            pltpu.VMEM((2, max_hops, slots, width), BF16),
            pltpu.VMEM((slots, width), BF16),
            pltpu.VMEM((slots, width), BF16),
            pltpu.VMEM((2, toks, slots), BF16),
            pltpu.SemaphoreType.REGULAR((nf,)),
            pltpu.SemaphoreType.REGULAR((4,)),
            dma((8,)),
            dma((4,)),
            dma,
            dma((CHUNKS,)),
            dma,
            dma((nf,)),
            dma,
            dma((nf,)),
            dma((2,)),
            dma((2,)),
            dma((2,)),
            dma((2, max_hops, CHUNKS)),
            dma,
            dma((CHUNKS,)),
            dma,
            dma((CHUNKS,)),
            dma,
            dma,
            dma((2,)),
            dma((2, max_hops, SUMS)),
            dma,
            dma,
        ],
        compiler_params=pltpu.CompilerParams(
            collective_id=0, has_side_effects=True, vmem_limit_bytes=60 * 1024 * 1024
        ),
        name="handover",
    )(
        tokens,
        route.T,
        group_weight.reshape(1, toks),
        pair_logit.reshape(1, toks),
        norm_gain.reshape(nf, rows_here),
        gate_train,
        up_train,
        down_train,
    )
    return (
        gate_serve.reshape(1, model, units),
        up_serve.reshape(1, model, units),
        down_serve.reshape(1, model, units),
        moe,
    )


def solution(mesh):
    nf, nt = mesh.shape["fs"], mesh.shape["tp"]
    pair = 2 if mesh.shape["grp"] % 2 == 0 else 1
    return jax.shard_map(
        functools.partial(shards, nf, nt, pair),
        mesh=mesh,
        in_specs=(
            P(("grp", "fs"), "tp"),
            P(("grp", "fs"), None),
            P(("grp", "fs")),
            P(("grp", "fs")),
            P(),
            P(None, "fs", "tp"),
            P(None, "fs", "tp"),
            P(None, "fs", "tp"),
        ),
        out_specs=(
            P(("grp", "fs"), None, "tp"),
            P(("grp", "fs"), None, "tp"),
            P(("grp", "fs"), None, "tp"),
            P(("grp", "fs"), "tp"),
        ),
        check_vma=False,
    )
```

```python
import functools

import jax
import jax.numpy as jnp
from jax import lax
from jax.experimental import pallas as pl
from jax.experimental.pallas import tpu as pltpu
from jax.sharding import PartitionSpec as P

CAP = 64
MESH = pl.DeviceIdType.MESH
F32 = jnp.float32
BF16 = jnp.bfloat16
CHUNKS = 4
PASS_FROM = 5
EARLY = 4
SUMS = 8
WAIT = (0, 0, 0, 0, 2, 2, 2, 2)


def ring_order(n):
    order = [n // 2]
    for far in range(n // 2 - 1, 0, -1):
        order += [far, n - far]
    return order + [0]


def dot(a, b, dims=(((1,), (0,)), ((), ()))):
    return lax.dot_general(a, b, dims, preferred_element_type=F32)


def body(
    nf,
    nx,
    pair,
    tokens_in,
    route_in,
    group_weight_in,
    pair_logit_in,
    gain_in,
    gate_in,
    up_in,
    down_in,
    gate_out,
    up_out,
    down_out,
    moe_out,
    tokens,
    route,
    group_weight,
    pair_logit,
    gain,
    stage_gu,
    stage_d,
    gain_col,
    send_tok,
    send_gu,
    send_d,
    section,
    w_gu,
    dw_own,
    dw_sib,
    h_own,
    h_sib,
    part,
    sums,
    ret,
    back,
    comb,
    ready,
    near,
    sem_in,
    sem_out,
    sem_tok_s,
    sem_tok_r,
    sem_gu_s,
    sem_gu_r,
    sem_d_s,
    sem_d_r,
    sem_y_s,
    sem_y_r,
    sem_x_s,
    sem_x_r,
    sem_c_s,
    sem_c_r,
    sem_h_s,
    sem_h_r,
    sem_w_s,
    sem_w_r,
    sem_q_s,
    sem_q_r,
    sem_b_s,
    sem_b_r,
):
    g, f, t = lax.axis_index("grp"), lax.axis_index("fs"), lax.axis_index("tp")
    x, c = t // 2, t % 2
    half = g % pair
    toks = tokens.shape[0]
    rows_here = gain_col.shape[0]
    rows_half = rows_here // pair
    model = nf * rows_here
    order = ring_order(nf)
    pos = {d: p for p, d in enumerate(order)}
    per = nf // CHUNKS
    chunk_rows = per * CAP
    max_hops = nx // 2

    def hops(ch, way):
        return max_hops - (ch + way) % 2

    def zdev(d):
        return (g, (f + d) % nf, t)

    along = ((g, f, ((x + 1) % nx) * 2 + c), (g, f, ((x + nx - 1) % nx) * 2 + c))
    sib = (g, f, x * 2 + 1 - c)
    twin = (g + 1 - 2 * half, f, t)

    def rows_of(ch):
        return pl.ds(ch * chunk_rows, chunk_rows)

    def remote(src, dst, s, r, dev):
        return pltpu.make_async_remote_copy(
            src_ref=src, dst_ref=dst, send_sem=s, recv_sem=r, device_id=dev, device_id_type=MESH
        )

    def drain(ref, s):
        pltpu.make_async_copy(ref, ref, s).wait()

    mine = pl.ds(half * rows_half, rows_half)
    small = [
        pltpu.make_async_copy(src, dst, sem_in.at[3 + i])
        for i, (src, dst) in enumerate(
            (
                (tokens_in, tokens),
                (route_in, route),
                (gain_in, gain),
                (group_weight_in, group_weight),
                (pair_logit_in, pair_logit),
            )
        )
    ]
    for cp in small:
        cp.start()
    loads = [
        pltpu.make_async_copy(gate_in.at[:, mine], stage_gu.at[0], sem_in.at[0]),
        pltpu.make_async_copy(up_in.at[:, mine], stage_gu.at[1], sem_in.at[1]),
        pltpu.make_async_copy(down_in.at[:, mine], stage_d, sem_in.at[2]),
    ]
    for cp in loads:
        cp.start()

    groups = lax.axis_size("grp")
    nt = 2 * nx
    late_first = ((groups - g) // groups) * ((nt - t) // nt)
    rank = (f + nf - late_first) % nf
    later_right = (x + 1) // nx
    earlier_left = (nx - x) // nx
    barrier = pltpu.get_barrier_semaphore()

    def greet(dev):
        pl.semaphore_signal(barrier, inc=1, device_id=dev, device_id_type=MESH)

    def tell(sem, dev):
        pl.semaphore_signal(sem, inc=1, device_id=dev, device_id_type=MESH)

    def if_later(d):
        return pl.when(rank + d < nf)

    def if_earlier(d):
        return pl.when(rank + d >= nf)

    for d in range(1, nf):
        if_later(d)(lambda d=d: greet(zdev(d)))
    pl.when(later_right == 1)(lambda: greet(along[0]))
    pl.when(earlier_left == 0)(lambda: greet(along[1]))
    pl.when(c == 1)(lambda: greet(sib))
    before = rank + (1 - later_right) + earlier_left + (1 - c)
    if pair == 2:
        pl.when(half == 1)(lambda: greet(twin))
        before = before + (1 - half)

    @pl.when(before > 0)
    def _():
        pl.semaphore_wait(barrier, before)

    for d in range(1, nf):
        if_earlier(d)(lambda d=d: tell(ready.at[nf - d], zdev(d)))
    pl.when(later_right == 0)(lambda: tell(near.at[1], along[0]))
    pl.when(earlier_left == 1)(lambda: tell(near.at[0], along[1]))
    pl.when(c == 0)(lambda: tell(near.at[2], sib))
    if pair == 2:
        pl.when(half == 0)(lambda: tell(near.at[3], twin))

    for cp in small:
        cp.wait()
    picked = route[...]
    rel = jnp.where(picked >= f, picked - f, picked - f + nf).astype(F32)
    first_t = jnp.broadcast_to(rel[0:1, :], (nf, toks))
    second_t = jnp.broadcast_to(rel[1:2, :], (nf, toks))
    offs = lax.broadcasted_iota(jnp.int32, (nf, toks), 0).astype(F32)
    hits_t = (first_t == offs) | (second_t == offs)
    ri = lax.broadcasted_iota(jnp.int32, (toks, toks), 0)
    ci = lax.broadcasted_iota(jnp.int32, (toks, toks), 1)
    upper = jnp.where(ri < ci, 1.0, 0.0).astype(BF16)
    rank_t = dot(jnp.where(hits_t, 1.0, 0.0).astype(BF16), upper)
    slot_t = jnp.where(hits_t, rank_t, -1.0)
    slots = lax.broadcasted_iota(jnp.int32, (CAP, toks), 0).astype(F32)
    for d in range(nf):
        pick = jnp.where(jnp.broadcast_to(slot_t[d : d + 1, :], (CAP, toks)) == slots, 1.0, 0.0)
        got = dot(pick.astype(BF16), tokens[...]).astype(BF16)
        if d == 0:
            section[t, pl.ds(pos[0] * CAP, CAP), :] = got
        else:
            send_tok[pl.ds(pos[d] * CAP, CAP), :] = got

    def w_rows(src):
        return pl.ds(pl.multiple_of(src * rows_here + half * rows_half, rows_half), rows_half)

    def d_at(src):
        return dw_own.at[(src + c) % 2, src // 2, mine]

    def send_rows(d):
        there = pos[(nf - d) % nf]
        remote(
            send_tok.at[pl.ds(pos[d] * CAP, CAP)],
            section.at[t, pl.ds(there * CAP, CAP)],
            sem_tok_s,
            sem_tok_r.at[there // per],
            zdev(d),
        ).start()

    def send_gate_up(d):
        remote(
            send_gu.at[(f + d) % nf], w_gu.at[w_rows(f)], sem_gu_s, sem_gu_r.at[f], zdev(d)
        ).start()

    def send_down(d):
        remote(
            send_d.at[(f + d) % nf], d_at(f), sem_d_s, sem_d_r.at[f], zdev(d)
        ).start()

    for d in order[:-1]:
        if_earlier(d)(lambda d=d: send_rows(d))

    gain_row = gain[pl.ds(f, 1), :]
    gain_col[...] = jnp.transpose(jnp.broadcast_to(gain_row, (rows_here, rows_here)))
    scale = gain_col[mine, :]
    loads[0].wait()
    loads[1].wait()

    def cast_gu(e, carry):
        send_gu[e, :, 0:128] = (scale * stage_gu[0, e]).astype(BF16)
        send_gu[e, :, 128:256] = (scale * stage_gu[1, e]).astype(BF16)
        return carry

    lax.fori_loop(0, nf, cast_gu, 0)
    w_gu[w_rows(f), :] = send_gu[f]
    loads[2].wait()

    def cast_d(e, carry):
        send_d[e] = stage_d[e].astype(BF16)
        return carry

    lax.fori_loop(0, nf, cast_d, 0)
    dw_own[(f + c) % 2, f // 2, mine, :] = send_d[f]

    first_in = nf // 2 + EARLY

    def send_weights(d):
        send_gate_up(d)
        send_down(d)

    def if_early(d):
        return pl.when((rank < first_in) & ((rank + d < first_in) | (rank + d >= nf)))

    def late(d):
        return (rank >= first_in) | ((rank + d < nf) & (rank + d >= first_in))

    def if_late(d):
        return pl.when(late(d))

    for d in order[:-1]:
        pl.when((rank + d >= nf) & (rank < first_in))(lambda d=d: send_weights(d))
    for d in range(1, nf):

        @if_later(d)
        def _(d=d):
            pl.semaphore_wait(ready.at[d], 1)
            send_rows(d)

        pl.when(rank + d < first_in)(lambda d=d: send_weights(d))

    def burst(guard):
        for step in (send_gate_up, send_down):
            for d in order[:-1]:
                pl.when(guard(d))(lambda d=d, step=step: step(d))

    burst(lambda d: rank == nf - 1)

    @pl.when(later_right == 1)
    def _():
        pl.semaphore_wait(near.at[0], 1)

    @pl.when(earlier_left == 0)
    def _():
        pl.semaphore_wait(near.at[1], 1)

    @pl.when(c == 1)
    def _():
        pl.semaphore_wait(near.at[2], 1)

    if pair == 2:

        @pl.when(half == 1)
        def _():
            pl.semaphore_wait(near.at[3], 1)

        remote(send_gu.at[f], w_gu.at[w_rows(f)], sem_y_s.at[0], sem_y_r.at[0], twin).start()
        remote(send_d.at[f], d_at(f), sem_y_s.at[1], sem_y_r.at[1], twin).start()

    def pass_gu(d):
        src = (f + d) % nf
        here = w_gu.at[w_rows(src)]
        remote(here, here, sem_y_s.at[0], sem_gu_r.at[src], twin).wait_recv()
        if pair == 2:
            remote(here, here, sem_y_s.at[0], sem_y_r.at[0], twin).start()

    def pass_d(d):
        src = (f + d) % nf
        here = d_at(src)
        remote(here, here, sem_y_s.at[1], sem_d_r.at[src], twin).wait_recv()
        if pair == 2:
            remote(here, here, sem_y_s.at[1], sem_y_r.at[1], twin).start()

    def gather_send(way, s, ch, blk):
        here = section.at[blk, rows_of(ch)]
        remote(here, here, sem_x_s.at[way], sem_x_r.at[way, s, ch], along[way]).start()

    def gather_share(ch, blk):
        here = section.at[blk, rows_of(ch)]
        remote(here, here, sem_c_s, sem_c_r.at[ch], sib).start()

    def gather_own(ch):
        count = per - (1 if pos[0] // per == ch else 0)
        drain(send_tok.at[pl.ds(0, count * CAP)], sem_tok_r.at[ch])
        for way in range(2):
            gather_send(way, 0, ch, t)
        gather_share(ch, t)

    def gather_step(s, ch):
        for way in range(2):
            if s > hops(ch, way):
                continue
            from_x = (x + (nx - s if way == 0 else s)) % nx
            blk = from_x * 2 + c
            here = section.at[blk, rows_of(ch)]
            remote(
                here, here, sem_x_s.at[way], sem_x_r.at[way, s - 1, ch], along[way]
            ).wait_recv()
            if s < hops(ch, way):
                gather_send(way, s, ch, blk)
            gather_share(ch, blk)

    def hidden(ch):
        drain(section.at[pl.ds(0, nx), pl.ds(0, chunk_rows)], sem_c_r.at[ch])
        blocks = [section[j, rows_of(ch), :] for j in range(2 * nx)]
        squares = jnp.zeros((chunk_rows, 128), F32)
        for b in blocks:
            wide = b.astype(F32)
            squares = squares + wide * wide
        row_scale = lax.rsqrt(jnp.sum(squares, axis=1, keepdims=True) / model + 1e-6)
        pre = dot(jnp.concatenate(blocks, axis=1), w_gu[...])
        gate = row_scale * pre[:, 0:128]
        up = row_scale * pre[:, 128:256]
        h_own[rows_of(ch), :] = (gate / (1.0 + jnp.exp(-gate)) * up).astype(BF16)
        remote(
            h_own.at[rows_of(ch)], h_sib.at[rows_of(ch)], sem_h_s, sem_h_r.at[ch], sib
        ).start()

    sum_rows = nf * CAP // SUMS
    per_sum = nf // SUMS

    def srows(u):
        return pl.ds(u * sum_rows, sum_rows)

    def sum_send(way, s, u, src):
        remote(
            src, sums.at[way, s, srows(u)], sem_q_s.at[way], sem_q_r.at[way, s, u], along[way]
        ).start()

    def target(way, u, s):
        left = hops(u, way) - s
        return (x + (left if way == 0 else nx - left)) % nx

    feats = nx * 128

    def partials(ch):
        remote(
            h_own.at[rows_of(ch)], h_sib.at[rows_of(ch)], sem_h_s, sem_h_r.at[ch], sib
        ).wait_recv()
        both = jnp.concatenate([h_own[rows_of(ch), :], h_sib[rows_of(ch), :]], axis=1)
        down = jnp.concatenate(
            [dw_own[0].reshape(feats, 128), dw_sib[...].reshape(feats, 128)], axis=1
        )
        res = dot(both, down, (((1,), (1,)), ((), ()))).astype(BF16)
        for i in range(nx):
            part[i, rows_of(ch), :] = res[:, i * 128 : (i + 1) * 128]

    def sum_step(s, u):
        for way in range(2):
            last = hops(u, way)
            if s > last:
                continue
            if s == 0:
                sum_send(way, 0, u, part.at[target(way, u, 0), srows(u)])
                continue
            here = sums.at[way, s - 1, srows(u)]
            remote(here, here, sem_q_s.at[way], sem_q_r.at[way, s - 1, u], along[way]).wait_recv()
            if s < last:
                sums[way, s - 1, srows(u), :] = (
                    sums[way, s - 1, srows(u), :].astype(F32)
                    + part[target(way, u, s), srows(u), :].astype(F32)
                ).astype(BF16)
                sum_send(way, s, u, here)
        if s < max_hops:
            return
        total = part[x, srows(u), :].astype(F32)
        for way in range(2):
            total = total + sums[way, hops(u, way) - 1, srows(u), :].astype(F32)
        ret[srows(u), :] = total.astype(BF16)
        for d in order[u * per_sum : (u + 1) * per_sum]:
            if d == 0:
                back[pl.ds(0, CAP), :] = ret[pl.ds(pos[0] * CAP, CAP), :]
            else:
                remote(
                    ret.at[pl.ds(pos[d] * CAP, CAP)],
                    back.at[pl.ds(((nf - d) % nf) * CAP, CAP)],
                    sem_b_s,
                    sem_b_r,
                    zdev(d),
                ).start()

    for ch in reversed(range(CHUNKS)):
        gather_own(ch)

    burst(lambda d: (rank < nf - 1) & late(d))
    for step in (pass_gu, pass_d):
        for d in order[:-1]:
            if_early(d)(lambda d=d, step=step: step(d))
    waiting = [(step, d) for step in (pass_gu, pass_d) for d in order[:-1]]
    event = 0
    for s in range(1, max_hops + 1):
        for ch in reversed(range(CHUNKS)):
            gather_step(s, ch)
            event += 1
            if event > PASS_FROM:
                for step, d in (waiting.pop(0), waiting.pop(0)):
                    if_late(d)(functools.partial(step, d))
    outs = [
        pltpu.make_async_copy(w_gu.at[:, pl.ds(0, 128)], gate_out, sem_out.at[0]),
        pltpu.make_async_copy(w_gu.at[:, pl.ds(128, 128)], up_out, sem_out.at[1]),
        pltpu.make_async_copy(dw_own.at[0], down_out.at[:, c], sem_out.at[2]),
        pltpu.make_async_copy(dw_own.at[1], down_out.at[:, 1 - c], sem_out.at[3]),
    ]
    for step, d in waiting:
        if_late(d)(functools.partial(step, d))
    if pair == 2:
        drain(w_gu.at[pl.ds(0, nf * rows_half)], sem_y_r.at[0])
    outs[0].start()
    outs[1].start()
    for ch in range(CHUNKS):
        hidden(ch)
    if pair == 2:
        drain(dw_own.at[0, :, pl.ds(0, nf * rows_half // nx)], sem_y_r.at[1])
    share = remote(dw_own.at[1], dw_sib, sem_w_s, sem_w_r, sib)
    share.start()
    outs[2].start()
    outs[3].start()
    share.wait_recv()
    for ch in range(CHUNKS):
        partials(ch)
        for u in range(ch * SUMS // CHUNKS, (ch + 1) * SUMS // CHUNKS):
            if WAIT[u] == 0:
                sum_step(0, u)

    lane = lax.broadcasted_iota(jnp.int32, (toks, 128), 1)
    lower = jnp.where(ci < ri, 1.0, 0.0).astype(BF16)
    first = jnp.transpose(jnp.broadcast_to(rel[0:1, :], (128, toks)))
    second = jnp.transpose(jnp.broadcast_to(rel[1:2, :], (128, toks)))
    weight = jnp.transpose(jnp.broadcast_to(group_weight[...], (128, toks)))
    logit = jnp.transpose(jnp.broadcast_to(pair_logit[...], (128, toks)))
    gate_a = weight * jax.nn.sigmoid(logit)
    gate_b = weight * jax.nn.sigmoid(-logit)
    lane_off = jnp.where(lane < CAP, 0, 1).astype(F32)
    lane_slot = jnp.where(lane < CAP, lane, lane - CAP).astype(F32)
    for k in range(nf // 2):
        off = lane_off + 2.0 * k
        is_a, is_b = first == off, second == off
        seen = dot(lower, jnp.where(is_a | is_b, 1.0, 0.0).astype(BF16))
        val = jnp.where(is_a, gate_a, 0.0) + jnp.where(is_b, gate_b, 0.0)
        val = jnp.where(seen == lane_slot, val, 0.0)
        high = val.astype(BF16)
        comb[0, :, pl.ds(k * 128, 128)] = high
        comb[1, :, pl.ds(k * 128, 128)] = (val - high.astype(F32)).astype(BF16)

    for k in range(1, max_hops + 1 + max(WAIT)):
        for u in range(SUMS):
            s = k - WAIT[u]
            if 0 <= s <= max_hops:
                sum_step(s, u)

    drain(back.at[pl.ds(0, (nf - 1) * CAP)], sem_b_r)
    rows_back = back[...]
    moe_out[...] = (dot(comb[0], rows_back) + dot(comb[1], rows_back)).astype(BF16)

    for cp in outs:
        cp.wait()
    drain(send_tok.at[pl.ds(0, (nf - 1) * CAP)], sem_tok_s)
    drain(send_gu.at[pl.ds(0, nf - 1)], sem_gu_s)
    drain(send_d.at[pl.ds(0, nf - 1)], sem_d_s)
    if pair == 2:
        drain(send_gu, sem_y_s.at[0])
        drain(send_d, sem_y_s.at[1])
    for way in range(2):
        moved = sum(hops(ch, way) for ch in range(CHUNKS))
        drain(section.at[pl.ds(0, moved), pl.ds(0, chunk_rows)], sem_x_s.at[way])
        moved = sum(hops(u, way) for u in range(SUMS))
        drain(section.at[pl.ds(0, nx // 2), pl.ds(0, moved * sum_rows // (nx // 2))], sem_q_s.at[way])
    drain(section.at[pl.ds(0, nx)], sem_c_s)
    drain(h_own, sem_h_s)
    share.wait_send()
    drain(ret.at[pl.ds(0, (nf - 1) * CAP)], sem_b_s)


def deliver(*refs):
    n = len(refs) // 3
    sources, outs, held = refs[:n], refs[n : 2 * n], refs[2 * n : 3 * n]
    sem_in, sem_out = refs[3 * n :]
    takes, gives = [], []
    for i in range(n):
        rows = sources[i].shape[0] // 2
        for part in range(2):
            at = pl.ds(part * rows, rows)
            k = 2 * i + part
            takes.append(pltpu.make_async_copy(sources[i].at[at], held[i].at[at], sem_in.at[k]))
            gives.append(pltpu.make_async_copy(held[i].at[at], outs[i].at[at], sem_out.at[k]))
    for cp in takes:
        cp.start()
    for take, give in zip(takes, gives):
        take.wait()
        give.start()
    for cp in gives:
        cp.wait()


def shards(
    nf, nt, pair, tokens, route, group_weight, pair_logit, norm_gain, gate_train, up_train, down_train
):
    nx = nt // 2
    toks, width = tokens.shape
    rows_here, units = gate_train.shape[1], gate_train.shape[2]
    rows_half = rows_here // pair
    model = norm_gain.shape[0]
    slots = nf * CAP
    max_hops = nx // 2
    vmem = pl.BlockSpec(memory_space=pltpu.VMEM)
    hbm = pl.BlockSpec(memory_space=pl.ANY)
    dma = pltpu.SemaphoreType.DMA
    gate_serve, up_serve, down_serve, moe = pl.pallas_call(
        functools.partial(body, nf, nx, pair),
        out_shape=(
            jax.ShapeDtypeStruct((model, units), BF16),
            jax.ShapeDtypeStruct((model, units), BF16),
            jax.ShapeDtypeStruct((nx, 2, rows_here, units), BF16),
            jax.ShapeDtypeStruct((toks, width), BF16),
        ),
        in_specs=[hbm] * 8,
        out_specs=(hbm, hbm, hbm, vmem),
        scratch_shapes=[
            pltpu.VMEM((toks, width), BF16),
            pltpu.VMEM((2, toks), jnp.int32),
            pltpu.VMEM((1, toks), F32),
            pltpu.VMEM((1, toks), F32),
            pltpu.VMEM((nf, rows_here), F32),
            pltpu.VMEM((2, nf, rows_half, units), F32),
            pltpu.VMEM((nf, rows_half, units), F32),
            pltpu.VMEM((rows_here, 128), F32),
            pltpu.VMEM((slots, width), BF16),
            pltpu.VMEM((nf, rows_half, 2 * units), BF16),
            pltpu.VMEM((nf, rows_half, units), BF16),
            pltpu.VMEM((nt, slots, width), BF16),
            pltpu.VMEM((model, 2 * units), BF16),
            pltpu.VMEM((2, nx, rows_here, units), BF16),
            pltpu.VMEM((nx, rows_here, units), BF16),
            pltpu.VMEM((slots, units), BF16),
            pltpu.VMEM((slots, units), BF16),
            pltpu.VMEM((nx, slots, width), BF16),
            pltpu.VMEM((2, max_hops, slots, width), BF16),
            pltpu.VMEM((slots, width), BF16),
            pltpu.VMEM((slots, width), BF16),
            pltpu.VMEM((2, toks, slots), BF16),
            pltpu.SemaphoreType.REGULAR((nf,)),
            pltpu.SemaphoreType.REGULAR((4,)),
            dma((8,)),
            dma((4,)),
            dma,
            dma((CHUNKS,)),
            dma,
            dma((nf,)),
            dma,
            dma((nf,)),
            dma((2,)),
            dma((2,)),
            dma((2,)),
            dma((2, max_hops, CHUNKS)),
            dma,
            dma((CHUNKS,)),
            dma,
            dma((CHUNKS,)),
            dma,
            dma,
            dma((2,)),
            dma((2, max_hops, SUMS)),
            dma,
            dma,
        ],
        compiler_params=pltpu.CompilerParams(
            collective_id=0, has_side_effects=True, vmem_limit_bytes=60 * 1024 * 1024
        ),
        name="handover",
    )(
        tokens,
        route.T,
        group_weight.reshape(1, toks),
        pair_logit.reshape(1, toks),
        norm_gain.reshape(nf, rows_here),
        gate_train,
        up_train,
        down_train,
    )
    made = (gate_serve, up_serve, down_serve, moe)
    gate_serve, up_serve, down_serve, moe = pl.pallas_call(
        deliver,
        out_shape=tuple(jax.ShapeDtypeStruct(a.shape, a.dtype) for a in made),
        in_specs=[hbm] * len(made),
        out_specs=(hbm,) * len(made),
        scratch_shapes=[pltpu.VMEM(a.shape, a.dtype) for a in made]
        + [dma((2 * len(made),)), dma((2 * len(made),))],
        compiler_params=pltpu.CompilerParams(vmem_limit_bytes=60 * 1024 * 1024),
        name="deliver",
    )(*made)
    return (
        gate_serve.reshape(1, model, units),
        up_serve.reshape(1, model, units),
        down_serve.reshape(1, model, units),
        moe,
    )


def solution(mesh):
    nf, nt = mesh.shape["fs"], mesh.shape["tp"]
    pair = 2 if mesh.shape["grp"] % 2 == 0 else 1
    return jax.shard_map(
        functools.partial(shards, nf, nt, pair),
        mesh=mesh,
        in_specs=(
            P(("grp", "fs"), "tp"),
            P(("grp", "fs"), None),
            P(("grp", "fs")),
            P(("grp", "fs")),
            P(),
            P(None, "fs", "tp"),
            P(None, "fs", "tp"),
            P(None, "fs", "tp"),
        ),
        out_specs=(
            P(("grp", "fs"), None, "tp"),
            P(("grp", "fs"), None, "tp"),
            P(("grp", "fs"), None, "tp"),
            P(("grp", "fs"), "tp"),
        ),
        check_vma=False,
    )
```

```python
import functools

import jax
import jax.numpy as jnp
from jax import lax
from jax.experimental import pallas as pl
from jax.experimental.pallas import tpu as pltpu
from jax.sharding import PartitionSpec as P

CAP = 64
MESH = pl.DeviceIdType.MESH
F32 = jnp.float32
BF16 = jnp.bfloat16
CHUNKS = 4
PASS_FROM = 8
EARLY = 4
SUMS = 8
WAIT = (0, 0, 0, 0, 2, 2, 2, 2)


def ring_order(n):
    order = [n // 2]
    for far in range(n // 2 - 1, 0, -1):
        order += [far, n - far]
    return order + [0]


def dot(a, b, dims=(((1,), (0,)), ((), ()))):
    return lax.dot_general(a, b, dims, preferred_element_type=F32)


def body(
    nf,
    nx,
    pair,
    tokens_in,
    route_in,
    group_weight_in,
    pair_logit_in,
    gain_in,
    gate_in,
    up_in,
    down_in,
    gate_out,
    up_out,
    down_out,
    moe_out,
    tokens,
    route,
    group_weight,
    pair_logit,
    gain,
    stage_gu,
    stage_d,
    gain_col,
    send_tok,
    send_gu,
    send_d,
    section,
    w_gu,
    dw_own,
    dw_sib,
    h_own,
    h_sib,
    part,
    sums,
    ret,
    back,
    comb,
    ready,
    near,
    sem_in,
    sem_out,
    sem_tok_s,
    sem_tok_r,
    sem_gu_s,
    sem_gu_r,
    sem_d_s,
    sem_d_r,
    sem_y_s,
    sem_y_r,
    sem_x_s,
    sem_x_r,
    sem_c_s,
    sem_c_r,
    sem_h_s,
    sem_h_r,
    sem_w_s,
    sem_w_r,
    sem_q_s,
    sem_q_r,
    sem_b_s,
    sem_b_r,
):
    g, f, t = lax.axis_index("grp"), lax.axis_index("fs"), lax.axis_index("tp")
    x, c = t // 2, t % 2
    half = g % pair
    toks = tokens.shape[0]
    rows_here = gain_col.shape[0]
    rows_half = rows_here // pair
    model = nf * rows_here
    order = ring_order(nf)
    pos = {d: p for p, d in enumerate(order)}
    per = nf // CHUNKS
    chunk_rows = per * CAP
    max_hops = nx // 2

    def hops(ch, way):
        return max_hops - (ch + way) % 2

    def zdev(d):
        return (g, (f + d) % nf, t)

    along = ((g, f, ((x + 1) % nx) * 2 + c), (g, f, ((x + nx - 1) % nx) * 2 + c))
    sib = (g, f, x * 2 + 1 - c)
    twin = (g + 1 - 2 * half, f, t)

    def rows_of(ch):
        return pl.ds(ch * chunk_rows, chunk_rows)

    def remote(src, dst, s, r, dev):
        return pltpu.make_async_remote_copy(
            src_ref=src, dst_ref=dst, send_sem=s, recv_sem=r, device_id=dev, device_id_type=MESH
        )

    def drain(ref, s):
        pltpu.make_async_copy(ref, ref, s).wait()

    mine = pl.ds(half * rows_half, rows_half)
    small = [
        pltpu.make_async_copy(src, dst, sem_in.at[3 + i])
        for i, (src, dst) in enumerate(
            (
                (tokens_in, tokens),
                (route_in, route),
                (gain_in, gain),
                (group_weight_in, group_weight),
                (pair_logit_in, pair_logit),
            )
        )
    ]
    for cp in small:
        cp.start()
    loads = [
        pltpu.make_async_copy(gate_in.at[:, mine], stage_gu.at[0], sem_in.at[0]),
        pltpu.make_async_copy(up_in.at[:, mine], stage_gu.at[1], sem_in.at[1]),
        pltpu.make_async_copy(down_in.at[:, mine], stage_d, sem_in.at[2]),
    ]
    for cp in loads:
        cp.start()

    groups = lax.axis_size("grp")
    nt = 2 * nx
    late_first = ((groups - g) // groups) * ((nt - t) // nt)
    rank = (f + nf - late_first) % nf
    later_right = (x + 1) // nx
    earlier_left = (nx - x) // nx
    barrier = pltpu.get_barrier_semaphore()

    def greet(dev):
        pl.semaphore_signal(barrier, inc=1, device_id=dev, device_id_type=MESH)

    def tell(sem, dev):
        pl.semaphore_signal(sem, inc=1, device_id=dev, device_id_type=MESH)

    def if_later(d):
        return pl.when(rank + d < nf)

    def if_earlier(d):
        return pl.when(rank + d >= nf)

    for d in range(1, nf):
        if_later(d)(lambda d=d: greet(zdev(d)))
    pl.when(later_right == 1)(lambda: greet(along[0]))
    pl.when(earlier_left == 0)(lambda: greet(along[1]))
    pl.when(c == 1)(lambda: greet(sib))
    before = rank + (1 - later_right) + earlier_left + (1 - c)
    if pair == 2:
        pl.when(half == 1)(lambda: greet(twin))
        before = before + (1 - half)

    @pl.when(before > 0)
    def _():
        pl.semaphore_wait(barrier, before)

    for d in range(1, nf):
        if_earlier(d)(lambda d=d: tell(ready.at[nf - d], zdev(d)))
    pl.when(later_right == 0)(lambda: tell(near.at[1], along[0]))
    pl.when(earlier_left == 1)(lambda: tell(near.at[0], along[1]))
    pl.when(c == 0)(lambda: tell(near.at[2], sib))
    if pair == 2:
        pl.when(half == 0)(lambda: tell(near.at[3], twin))

    for cp in small:
        cp.wait()
    picked = route[...]
    rel = jnp.where(picked >= f, picked - f, picked - f + nf).astype(F32)
    first_t = jnp.broadcast_to(rel[0:1, :], (nf, toks))
    second_t = jnp.broadcast_to(rel[1:2, :], (nf, toks))
    offs = lax.broadcasted_iota(jnp.int32, (nf, toks), 0).astype(F32)
    hits_t = (first_t == offs) | (second_t == offs)
    ri = lax.broadcasted_iota(jnp.int32, (toks, toks), 0)
    ci = lax.broadcasted_iota(jnp.int32, (toks, toks), 1)
    upper = jnp.where(ri < ci, 1.0, 0.0).astype(BF16)
    rank_t = dot(jnp.where(hits_t, 1.0, 0.0).astype(BF16), upper)
    slot_t = jnp.where(hits_t, rank_t, -1.0)
    slots = lax.broadcasted_iota(jnp.int32, (CAP, toks), 0).astype(F32)
    for d in range(nf):
        pick = jnp.where(jnp.broadcast_to(slot_t[d : d + 1, :], (CAP, toks)) == slots, 1.0, 0.0)
        got = dot(pick.astype(BF16), tokens[...]).astype(BF16)
        if d == 0:
            section[t, pl.ds(pos[0] * CAP, CAP), :] = got
        else:
            send_tok[pl.ds(pos[d] * CAP, CAP), :] = got

    def w_rows(src):
        return pl.ds(pl.multiple_of(src * rows_here + half * rows_half, rows_half), rows_half)

    def d_at(src):
        return dw_own.at[(src + c) % 2, src // 2, mine]

    def send_rows(d):
        there = pos[(nf - d) % nf]
        remote(
            send_tok.at[pl.ds(pos[d] * CAP, CAP)],
            section.at[t, pl.ds(there * CAP, CAP)],
            sem_tok_s,
            sem_tok_r.at[there // per],
            zdev(d),
        ).start()

    def send_gate_up(d):
        remote(
            send_gu.at[(f + d) % nf], w_gu.at[w_rows(f)], sem_gu_s, sem_gu_r.at[f], zdev(d)
        ).start()

    def send_down(d):
        remote(
            send_d.at[(f + d) % nf], d_at(f), sem_d_s, sem_d_r.at[f], zdev(d)
        ).start()

    for d in order[:-1]:
        if_earlier(d)(lambda d=d: send_rows(d))

    gain_row = gain[pl.ds(f, 1), :]
    gain_col[...] = jnp.transpose(jnp.broadcast_to(gain_row, (rows_here, rows_here)))
    scale = gain_col[mine, :]
    loads[0].wait()
    loads[1].wait()

    def cast_gu(e, carry):
        send_gu[e, :, 0:128] = (scale * stage_gu[0, e]).astype(BF16)
        send_gu[e, :, 128:256] = (scale * stage_gu[1, e]).astype(BF16)
        return carry

    lax.fori_loop(0, nf, cast_gu, 0)
    w_gu[w_rows(f), :] = send_gu[f]
    loads[2].wait()

    def cast_d(e, carry):
        send_d[e] = stage_d[e].astype(BF16)
        return carry

    lax.fori_loop(0, nf, cast_d, 0)
    dw_own[(f + c) % 2, f // 2, mine, :] = send_d[f]

    first_in = nf // 2 + EARLY

    def send_weights(d):
        send_gate_up(d)
        send_down(d)

    def if_early(d):
        return pl.when((rank < first_in) & ((rank + d < first_in) | (rank + d >= nf)))

    def late(d):
        return (rank >= first_in) | ((rank + d < nf) & (rank + d >= first_in))

    def if_late(d):
        return pl.when(late(d))

    for d in order[:-1]:
        pl.when((rank + d >= nf) & (rank < first_in))(lambda d=d: send_weights(d))
    for d in range(1, nf):

        @if_later(d)
        def _(d=d):
            pl.semaphore_wait(ready.at[d], 1)
            send_rows(d)

        pl.when(rank + d < first_in)(lambda d=d: send_weights(d))

    def burst(guard):
        for step in (send_gate_up, send_down):
            for d in order[:-1]:
                pl.when(guard(d))(lambda d=d, step=step: step(d))

    burst(lambda d: rank == nf - 1)

    @pl.when(later_right == 1)
    def _():
        pl.semaphore_wait(near.at[0], 1)

    @pl.when(earlier_left == 0)
    def _():
        pl.semaphore_wait(near.at[1], 1)

    @pl.when(c == 1)
    def _():
        pl.semaphore_wait(near.at[2], 1)

    if pair == 2:

        @pl.when(half == 1)
        def _():
            pl.semaphore_wait(near.at[3], 1)

        remote(send_gu.at[f], w_gu.at[w_rows(f)], sem_y_s.at[0], sem_y_r.at[0], twin).start()
        remote(send_d.at[f], d_at(f), sem_y_s.at[1], sem_y_r.at[1], twin).start()

    def pass_gu(d):
        src = (f + d) % nf
        here = w_gu.at[w_rows(src)]
        remote(here, here, sem_y_s.at[0], sem_gu_r.at[src], twin).wait_recv()
        if pair == 2:
            remote(here, here, sem_y_s.at[0], sem_y_r.at[0], twin).start()

    def pass_d(d):
        src = (f + d) % nf
        here = d_at(src)
        remote(here, here, sem_y_s.at[1], sem_d_r.at[src], twin).wait_recv()
        if pair == 2:
            remote(here, here, sem_y_s.at[1], sem_y_r.at[1], twin).start()

    def gather_send(way, s, ch, blk):
        here = section.at[blk, rows_of(ch)]
        remote(here, here, sem_x_s.at[way], sem_x_r.at[way, s, ch], along[way]).start()

    def gather_share(ch, blk):
        here = section.at[blk, rows_of(ch)]
        remote(here, here, sem_c_s, sem_c_r.at[ch], sib).start()

    def gather_own(ch):
        count = per - (1 if pos[0] // per == ch else 0)
        drain(send_tok.at[pl.ds(0, count * CAP)], sem_tok_r.at[ch])
        for way in range(2):
            gather_send(way, 0, ch, t)
        gather_share(ch, t)

    def gather_step(s, ch):
        for way in range(2):
            if s > hops(ch, way):
                continue
            from_x = (x + (nx - s if way == 0 else s)) % nx
            blk = from_x * 2 + c
            here = section.at[blk, rows_of(ch)]
            remote(
                here, here, sem_x_s.at[way], sem_x_r.at[way, s - 1, ch], along[way]
            ).wait_recv()
            if s < hops(ch, way):
                gather_send(way, s, ch, blk)
            gather_share(ch, blk)

    def hidden(ch):
        drain(section.at[pl.ds(0, nx), pl.ds(0, chunk_rows)], sem_c_r.at[ch])
        blocks = [section[j, rows_of(ch), :] for j in range(2 * nx)]
        squares = jnp.zeros((chunk_rows, 128), F32)
        for b in blocks:
            wide = b.astype(F32)
            squares = squares + wide * wide
        row_scale = lax.rsqrt(jnp.sum(squares, axis=1, keepdims=True) / model + 1e-6)
        pre = dot(jnp.concatenate(blocks, axis=1), w_gu[...])
        gate = row_scale * pre[:, 0:128]
        up = row_scale * pre[:, 128:256]
        h_own[rows_of(ch), :] = (gate / (1.0 + jnp.exp(-gate)) * up).astype(BF16)
        remote(
            h_own.at[rows_of(ch)], h_sib.at[rows_of(ch)], sem_h_s, sem_h_r.at[ch], sib
        ).start()

    sum_rows = nf * CAP // SUMS
    per_sum = nf // SUMS

    def srows(u):
        return pl.ds(u * sum_rows, sum_rows)

    def sum_send(way, s, u, src):
        remote(
            src, sums.at[way, s, srows(u)], sem_q_s.at[way], sem_q_r.at[way, s, u], along[way]
        ).start()

    def target(way, u, s):
        left = hops(u, way) - s
        return (x + (left if way == 0 else nx - left)) % nx

    feats = nx * 128

    def partials(ch):
        remote(
            h_own.at[rows_of(ch)], h_sib.at[rows_of(ch)], sem_h_s, sem_h_r.at[ch], sib
        ).wait_recv()
        both = jnp.concatenate([h_own[rows_of(ch), :], h_sib[rows_of(ch), :]], axis=1)
        down = jnp.concatenate(
            [dw_own[0].reshape(feats, 128), dw_sib[...].reshape(feats, 128)], axis=1
        )
        res = dot(both, down, (((1,), (1,)), ((), ()))).astype(BF16)
        for i in range(nx):
            part[i, rows_of(ch), :] = res[:, i * 128 : (i + 1) * 128]

    def sum_step(s, u):
        for way in range(2):
            last = hops(u, way)
            if s > last:
                continue
            if s == 0:
                sum_send(way, 0, u, part.at[target(way, u, 0), srows(u)])
                continue
            here = sums.at[way, s - 1, srows(u)]
            remote(here, here, sem_q_s.at[way], sem_q_r.at[way, s - 1, u], along[way]).wait_recv()
            if s < last:
                sums[way, s - 1, srows(u), :] = (
                    sums[way, s - 1, srows(u), :].astype(F32)
                    + part[target(way, u, s), srows(u), :].astype(F32)
                ).astype(BF16)
                sum_send(way, s, u, here)
        if s < max_hops:
            return
        total = part[x, srows(u), :].astype(F32)
        for way in range(2):
            total = total + sums[way, hops(u, way) - 1, srows(u), :].astype(F32)
        ret[srows(u), :] = total.astype(BF16)
        for d in order[u * per_sum : (u + 1) * per_sum]:
            if d == 0:
                back[pl.ds(0, CAP), :] = ret[pl.ds(pos[0] * CAP, CAP), :]
            else:
                remote(
                    ret.at[pl.ds(pos[d] * CAP, CAP)],
                    back.at[pl.ds(((nf - d) % nf) * CAP, CAP)],
                    sem_b_s,
                    sem_b_r,
                    zdev(d),
                ).start()

    for ch in reversed(range(CHUNKS)):
        gather_own(ch)

    burst(lambda d: (rank < nf - 1) & late(d))
    for step in (pass_gu, pass_d):
        for d in order[:-1]:
            if_early(d)(lambda d=d, step=step: step(d))
    waiting = [(step, d) for step in (pass_gu, pass_d) for d in order[:-1]]
    event = 0
    for s in range(1, max_hops + 1):
        for ch in reversed(range(CHUNKS)):
            gather_step(s, ch)
            event += 1
            if event > PASS_FROM:
                for step, d in (waiting.pop(0), waiting.pop(0)):
                    if_late(d)(functools.partial(step, d))
    outs = [
        pltpu.make_async_copy(w_gu.at[:, pl.ds(0, 128)], gate_out, sem_out.at[0]),
        pltpu.make_async_copy(w_gu.at[:, pl.ds(128, 128)], up_out, sem_out.at[1]),
        pltpu.make_async_copy(dw_own.at[0], down_out.at[:, c], sem_out.at[2]),
        pltpu.make_async_copy(dw_own.at[1], down_out.at[:, 1 - c], sem_out.at[3]),
    ]
    for step, d in waiting:
        if_late(d)(functools.partial(step, d))
    if pair == 2:
        drain(w_gu.at[pl.ds(0, nf * rows_half)], sem_y_r.at[0])
    outs[0].start()
    outs[1].start()
    for ch in range(CHUNKS):
        hidden(ch)
    if pair == 2:
        drain(dw_own.at[0, :, pl.ds(0, nf * rows_half // nx)], sem_y_r.at[1])
    share = remote(dw_own.at[1], dw_sib, sem_w_s, sem_w_r, sib)
    share.start()
    outs[2].start()
    outs[3].start()
    share.wait_recv()
    for ch in range(CHUNKS):
        partials(ch)
        for u in range(ch * SUMS // CHUNKS, (ch + 1) * SUMS // CHUNKS):
            if WAIT[u] == 0:
                sum_step(0, u)

    lane = lax.broadcasted_iota(jnp.int32, (toks, 128), 1)
    lower = jnp.where(ci < ri, 1.0, 0.0).astype(BF16)
    first = jnp.transpose(jnp.broadcast_to(rel[0:1, :], (128, toks)))
    second = jnp.transpose(jnp.broadcast_to(rel[1:2, :], (128, toks)))
    weight = jnp.transpose(jnp.broadcast_to(group_weight[...], (128, toks)))
    logit = jnp.transpose(jnp.broadcast_to(pair_logit[...], (128, toks)))
    gate_a = weight * jax.nn.sigmoid(logit)
    gate_b = weight * jax.nn.sigmoid(-logit)
    lane_off = jnp.where(lane < CAP, 0, 1).astype(F32)
    lane_slot = jnp.where(lane < CAP, lane, lane - CAP).astype(F32)
    for k in range(nf // 2):
        off = lane_off + 2.0 * k
        is_a, is_b = first == off, second == off
        seen = dot(lower, jnp.where(is_a | is_b, 1.0, 0.0).astype(BF16))
        val = jnp.where(is_a, gate_a, 0.0) + jnp.where(is_b, gate_b, 0.0)
        val = jnp.where(seen == lane_slot, val, 0.0)
        high = val.astype(BF16)
        comb[0, :, pl.ds(k * 128, 128)] = high
        comb[1, :, pl.ds(k * 128, 128)] = (val - high.astype(F32)).astype(BF16)

    for k in range(1, max_hops + 1 + max(WAIT)):
        for u in range(SUMS):
            s = k - WAIT[u]
            if 0 <= s <= max_hops:
                sum_step(s, u)

    drain(back.at[pl.ds(0, (nf - 1) * CAP)], sem_b_r)
    rows_back = back[...]
    moe_out[...] = (dot(comb[0], rows_back) + dot(comb[1], rows_back)).astype(BF16)

    for cp in outs:
        cp.wait()
    drain(send_tok.at[pl.ds(0, (nf - 1) * CAP)], sem_tok_s)
    drain(send_gu.at[pl.ds(0, nf - 1)], sem_gu_s)
    drain(send_d.at[pl.ds(0, nf - 1)], sem_d_s)
    if pair == 2:
        drain(send_gu, sem_y_s.at[0])
        drain(send_d, sem_y_s.at[1])
    for way in range(2):
        moved = sum(hops(ch, way) for ch in range(CHUNKS))
        drain(section.at[pl.ds(0, moved), pl.ds(0, chunk_rows)], sem_x_s.at[way])
        moved = sum(hops(u, way) for u in range(SUMS))
        drain(section.at[pl.ds(0, nx // 2), pl.ds(0, moved * sum_rows // (nx // 2))], sem_q_s.at[way])
    drain(section.at[pl.ds(0, nx)], sem_c_s)
    drain(h_own, sem_h_s)
    share.wait_send()
    drain(ret.at[pl.ds(0, (nf - 1) * CAP)], sem_b_s)


def deliver(*refs):
    n = len(refs) // 3
    sources, outs, held = refs[:n], refs[n : 2 * n], refs[2 * n : 3 * n]
    sem_in, sem_out = refs[3 * n :]
    takes, gives = [], []
    for i in range(n):
        rows = sources[i].shape[0] // 2
        for part in range(2):
            at = pl.ds(part * rows, rows)
            k = 2 * i + part
            takes.append(pltpu.make_async_copy(sources[i].at[at], held[i].at[at], sem_in.at[k]))
            gives.append(pltpu.make_async_copy(held[i].at[at], outs[i].at[at], sem_out.at[k]))
    for cp in takes:
        cp.start()
    for take, give in zip(takes, gives):
        take.wait()
        give.start()
    for cp in gives:
        cp.wait()


def shards(
    nf, nt, pair, tokens, route, group_weight, pair_logit, norm_gain, gate_train, up_train, down_train
):
    nx = nt // 2
    toks, width = tokens.shape
    rows_here, units = gate_train.shape[1], gate_train.shape[2]
    rows_half = rows_here // pair
    model = norm_gain.shape[0]
    slots = nf * CAP
    max_hops = nx // 2
    vmem = pl.BlockSpec(memory_space=pltpu.VMEM)
    hbm = pl.BlockSpec(memory_space=pl.ANY)
    dma = pltpu.SemaphoreType.DMA
    gate_serve, up_serve, down_serve, moe = pl.pallas_call(
        functools.partial(body, nf, nx, pair),
        out_shape=(
            jax.ShapeDtypeStruct((model, units), BF16),
            jax.ShapeDtypeStruct((model, units), BF16),
            jax.ShapeDtypeStruct((nx, 2, rows_here, units), BF16),
            jax.ShapeDtypeStruct((toks, width), BF16),
        ),
        in_specs=[hbm] * 8,
        out_specs=(hbm, hbm, hbm, vmem),
        scratch_shapes=[
            pltpu.VMEM((toks, width), BF16),
            pltpu.VMEM((2, toks), jnp.int32),
            pltpu.VMEM((1, toks), F32),
            pltpu.VMEM((1, toks), F32),
            pltpu.VMEM((nf, rows_here), F32),
            pltpu.VMEM((2, nf, rows_half, units), F32),
            pltpu.VMEM((nf, rows_half, units), F32),
            pltpu.VMEM((rows_here, 128), F32),
            pltpu.VMEM((slots, width), BF16),
            pltpu.VMEM((nf, rows_half, 2 * units), BF16),
            pltpu.VMEM((nf, rows_half, units), BF16),
            pltpu.VMEM((nt, slots, width), BF16),
            pltpu.VMEM((model, 2 * units), BF16),
            pltpu.VMEM((2, nx, rows_here, units), BF16),
            pltpu.VMEM((nx, rows_here, units), BF16),
            pltpu.VMEM((slots, units), BF16),
            pltpu.VMEM((slots, units), BF16),
            pltpu.VMEM((nx, slots, width), BF16),
            pltpu.VMEM((2, max_hops, slots, width), BF16),
            pltpu.VMEM((slots, width), BF16),
            pltpu.VMEM((slots, width), BF16),
            pltpu.VMEM((2, toks, slots), BF16),
            pltpu.SemaphoreType.REGULAR((nf,)),
            pltpu.SemaphoreType.REGULAR((4,)),
            dma((8,)),
            dma((4,)),
            dma,
            dma((CHUNKS,)),
            dma,
            dma((nf,)),
            dma,
            dma((nf,)),
            dma((2,)),
            dma((2,)),
            dma((2,)),
            dma((2, max_hops, CHUNKS)),
            dma,
            dma((CHUNKS,)),
            dma,
            dma((CHUNKS,)),
            dma,
            dma,
            dma((2,)),
            dma((2, max_hops, SUMS)),
            dma,
            dma,
        ],
        compiler_params=pltpu.CompilerParams(
            collective_id=0, has_side_effects=True, vmem_limit_bytes=60 * 1024 * 1024
        ),
        name="handover",
    )(
        tokens,
        route.T,
        group_weight.reshape(1, toks),
        pair_logit.reshape(1, toks),
        norm_gain.reshape(nf, rows_here),
        gate_train,
        up_train,
        down_train,
    )
    made = (gate_serve, up_serve, down_serve, moe)
    gate_serve, up_serve, down_serve, moe = pl.pallas_call(
        deliver,
        out_shape=tuple(jax.ShapeDtypeStruct(a.shape, a.dtype) for a in made),
        in_specs=[hbm] * len(made),
        out_specs=(hbm,) * len(made),
        scratch_shapes=[pltpu.VMEM(a.shape, a.dtype) for a in made]
        + [dma((2 * len(made),)), dma((2 * len(made),))],
        compiler_params=pltpu.CompilerParams(vmem_limit_bytes=60 * 1024 * 1024),
        name="deliver",
    )(*made)
    return (
        gate_serve.reshape(1, model, units),
        up_serve.reshape(1, model, units),
        down_serve.reshape(1, model, units),
        moe,
    )


def solution(mesh):
    nf, nt = mesh.shape["fs"], mesh.shape["tp"]
    pair = 2 if mesh.shape["grp"] % 2 == 0 else 1
    return jax.shard_map(
        functools.partial(shards, nf, nt, pair),
        mesh=mesh,
        in_specs=(
            P(("grp", "fs"), "tp"),
            P(("grp", "fs"), None),
            P(("grp", "fs")),
            P(("grp", "fs")),
            P(),
            P(None, "fs", "tp"),
            P(None, "fs", "tp"),
            P(None, "fs", "tp"),
        ),
        out_specs=(
            P(("grp", "fs"), None, "tp"),
            P(("grp", "fs"), None, "tp"),
            P(("grp", "fs"), None, "tp"),
            P(("grp", "fs"), "tp"),
        ),
        check_vma=False,
    )
```
